512 devices in a mesh: fs: 128 (over z, y, core), tp: 4 (over x).
Axes of the slice: x: 4, y: 8, z: 8, core: 2. Of those that a mesh axis runs over, the one named last changes fastest.
Arguments:
- query_one: bfloat16 [81920, 1024], P('fs', 'tp'), as said below
- key_one: bfloat16 [81920, 1024], P('fs', 'tp'), as said below
- query_two: bfloat16 [81920, 1024], P('fs', 'tp'), as said below
- key_two: bfloat16 [81920, 1024], P('fs', 'tp'), as said below
- values: bfloat16 [81920, 2048], P('fs', 'tp'), may hold values from -6 to 6
- mix_ratio: float32 [8], P('tp'), may hold values from 0.3 to 0.8
- head_gain: float32 [256], replicated, may hold values from 0.1 to 1.9
- cotangent: bfloat16 [81920, 2048], P('fs', 'tp'), may hold values from -0.1875 to 0.1875
- left_roots: bfloat16 [2048, 2048], P('fs'), as said below
- right_roots: bfloat16 [2048, 256], P('tp'), as said below
- weight: float32 [2048, 2048], P('fs', 'tp'), may hold values from -3 to 3
- momentum: float32 [2048, 2048], P('fs', 'tp'), as said below
Outputs:
- update_step: float32 [2048, 2048], P('fs', 'tp')
- weight_new: float32 [2048, 2048], P('fs', 'tp')
- momentum_new: float32 [2048, 2048], P('fs', 'tp')
- weight_copy: bfloat16 [2048, 2048], P(None, 'tp')
The draws below stay inside these ranges and needn't reach their ends.
Inputs may be any that keep to these rules, and one draw needn't show every extreme that they name: `query_one`: Real-valued. `key_one`: Real-valued. `query_two`: Real-valued. `key_two`: Real-valued. `left_roots`: Real-valued. `right_roots`: Real-valued. `momentum`: Real-valued.
All inputs are finite; a program needn't handle non-finite values.
Results may differ from the reference program's by a relative error of at most 0.0039.
Values may be sent and summed in bfloat16 or wider, within the bound.
A program may use at most 64 MiB of HBM per device.

```python
import jax
import jax.numpy as jnp
from jax import lax

D = 2048
HEADS = 8
DK = 128
DV = 256
TOK_DEV = 640
HV = 2048
TOKENS = 81920
N_FS = 128


def drawn(key, salt):
    base = jax.random.fold_in(key, salt)
    width = HEADS * DK
    query = 1.3 * jax.random.truncated_normal(jax.random.fold_in(base, 1), -6.0, 6.0, (TOKENS, width), jnp.float32)
    keys = 1.3 * jax.random.truncated_normal(jax.random.fold_in(base, 2), -6.0, 6.0, (TOKENS, width), jnp.float32)
    return (query, keys)


def draw_query_one(key, part):
    return drawn(key, 11)[0].astype(jnp.bfloat16)


def draw_key_one(key, part):
    return drawn(key, 11)[1].astype(jnp.bfloat16)


def draw_query_two(key, part):
    return drawn(key, 12)[0].astype(jnp.bfloat16)


def draw_key_two(key, part):
    return drawn(key, 12)[1].astype(jnp.bfloat16)


def roots(key, count, size):
    noise = jax.random.normal(jax.random.fold_in(key, 21), (count, size, size), jnp.float32)
    symmetric = (noise + jnp.swapaxes(noise, 1, 2)) * 0.5 / (2.0 * size) ** 0.5
    diagonal = jax.random.uniform(jax.random.fold_in(key, 22), (count, size), jnp.float32, 1.0, 2.0)
    return symmetric + diagonal[:, :, None] * jnp.eye(size, dtype=jnp.float32)[None, :, :]


def draw_left_roots(key, part):
    return roots(key, 1, D).reshape(D, D).astype(jnp.bfloat16)


def draw_right_roots(key, part):
    return roots(key, HEADS, DV).reshape(HEADS * DV, DV).astype(jnp.bfloat16)


def draw_momentum(key, part):
    rows = 0.3 * (1.0 + 4.0 * jnp.arange(D, dtype=jnp.float32) / D)
    columns = 1.0 + 2.0 * jnp.arange(HV, dtype=jnp.float32) / HV
    base = jax.random.normal(key, (D, HV), jnp.float32)
    scales = rows[:, None] * columns[None, :]
    return base * scales


def spiked(result, own_key, source, target, blocks, factor):
    def block_of(axis_at):
        return (jnp.arange(result.shape[axis_at]) // (result.shape[axis_at] // blocks)).reshape((-1,) + (1,) * (result.ndim - 1 - axis_at))

    first = jax.random.permutation(own_key, blocks)[block_of(target)]
    other_side = (block_of(target) + blocks // 2) % blocks
    return jnp.where((block_of(source) == first) | (block_of(source) == other_side), factor * result, result)


def shard_levels(rng, extent, split, smallest, largest):
    factor_of = 1.0
    for dim, blocks in split:
        heights = jax.random.uniform(jax.random.fold_in(jax.random.fold_in(rng, 6), dim), (blocks,), jnp.float32, smallest / len(split), largest / len(split))
        factor_of = factor_of * jnp.repeat(jnp.exp(heights), extent[dim] // blocks).reshape((-1,) + (1,) * (len(extent) - 1 - dim))
    return factor_of


def gaussian(stream_key, dims, deviation, most, split=(), kind=jnp.bfloat16):
    level = shard_levels(stream_key, dims, split, -0.22, 0.18) if split else 1.0
    result = jax.random.normal(stream_key, dims, jnp.float32) * deviation * level
    return jnp.minimum(jnp.maximum(result, -most), most).astype(kind)


def noise_with(own_key, extent, spread, bound, split, heavy, kind=jnp.bfloat16):
    drawn = spread * jax.random.normal(own_key, extent, jnp.float32)
    if split:
        drawn = drawn * shard_levels(own_key, extent, split, -0.22, 0.18)
    return jnp.clip(spiked(drawn, jax.random.fold_in(own_key, 3), *heavy), -bound, bound).astype(kind)


def setup_inputs(seed: int = 0) -> dict:
    key_of = jax.random.split(jax.random.key(seed), 13)
    return {
        "query_one": draw_query_one(jax.random.fold_in(key_of[12], 71), 0),
        "key_one": draw_key_one(jax.random.fold_in(key_of[12], 71), 0),
        "query_two": draw_query_two(jax.random.fold_in(key_of[12], 71), 0),
        "key_two": draw_key_two(jax.random.fold_in(key_of[12], 71), 0),
        "values": gaussian(key_of[4], (TOKENS, HV), 1.0, 6.0, ((0, 128), (1, 4))),
        "mix_ratio": jnp.clip(0.3 + 0.5 * jax.random.uniform(key_of[5], (HEADS,), jnp.float32) ** shard_levels(key_of[5], (HEADS,), ((0, 4),), -0.2, 0.2), 0.3, 0.8),
        "head_gain": jnp.clip(1.0 + 0.18 * jax.random.normal(key_of[6], (DV,), jnp.float32), 0.1, 1.9),
        "cotangent": noise_with(key_of[7], (TOKENS, D), ((TOK_DEV * N_FS) ** -0.5), 0.1875, ((0, 128), (1, 4)), (0, 1, 128, 5.5)),
        "left_roots": draw_left_roots(jax.random.fold_in(key_of[12], 71), 0),
        "right_roots": draw_right_roots(jax.random.fold_in(key_of[12], 71), 0),
        "weight": gaussian(key_of[10], (D, HV), 0.5, 3.0, ((0, 128), (1, 4)), jnp.float32),
        "momentum": draw_momentum(jax.random.fold_in(key_of[12], 71), 0),
    }


epsilon = 1e-06
momentum_decay = 0.8
clip_level = 0.5
weight_decay = 0.2
step_rate = 0.1

def attend(query_one, key_one, query_two, key_two, values, mix_ratio, head_gain):
    count = TOKENS // TOK_DEV
    causal = jnp.tril(jnp.ones((TOK_DEV, TOK_DEV), dtype=bool))

    def probs(query, keys):
        scores = jnp.einsum('qhd,khd->hqk', query.astype(jnp.float32), keys.astype(jnp.float32)) * DK ** (-0.5)
        return jax.nn.softmax(jnp.where(causal, scores, -jnp.inf), axis=-1)

    def one_sequence(item):
        first_q, first_k, second_q, second_k, vals = item
        mixed = (probs(first_q, first_k) - mix_ratio[:, None, None] * probs(second_q, second_k)).astype(jnp.bfloat16)
        head_out = jnp.einsum('hqk,khd->qhd', mixed.astype(jnp.float32), vals.astype(jnp.float32))
        square = lax.optimization_barrier(jnp.mean(head_out * head_out, axis=-1, keepdims=True))
        normed = head_out * lax.rsqrt(square + epsilon) * head_gain
        return normed.astype(jnp.bfloat16).reshape(TOK_DEV, HV)
    shaped = (query_one.reshape(count, TOK_DEV, HEADS, DK), key_one.reshape(count, TOK_DEV, HEADS, DK), query_two.reshape(count, TOK_DEV, HEADS, DK), key_two.reshape(count, TOK_DEV, HEADS, DK), values.reshape(count, TOK_DEV, HEADS, DV))
    return lax.map(one_sequence, shaped).reshape(TOKENS, HV)

def reference(query_one, key_one, query_two, key_two, values, mix_ratio, head_gain, cotangent, left_roots, right_roots, weight, momentum):
    attended = attend(query_one, key_one, query_two, key_two, values, mix_ratio, head_gain)
    gradient = jnp.dot(cotangent.T, attended, preferred_element_type=jnp.float32)
    left_done = jnp.dot(left_roots.astype(jnp.float32), gradient, precision=lax.Precision.HIGHEST, preferred_element_type=jnp.float32)
    right_full = right_roots.astype(jnp.float32).reshape(HEADS, DV, DV)
    preconditioned = jnp.einsum('dhc,hce->dhe', left_done.reshape(D, HEADS, DV), right_full, precision=lax.Precision.HIGHEST).reshape(D, HV)
    momentum_new = momentum_decay * momentum + (1.0 - momentum_decay) * preconditioned
    total = jnp.sum(momentum_new * momentum_new)
    factor = clip_level * lax.rsqrt(total / (D * HV) + epsilon)
    update_step = factor * momentum_new + weight_decay * weight
    weight_new = weight - step_rate * update_step
    return (update_step, weight_new, momentum_new, weight_new.astype(jnp.bfloat16))
```

```python
import functools

import jax
import jax.numpy as jnp
from jax import lax
from jax.experimental import pallas as pl
from jax.experimental.pallas import tpu as pltpu
from jax.sharding import Mesh
from jax.sharding import PartitionSpec as P

FS = ("fs_0", "fs_1", "fs_2")
MESH_ID = pl.DeviceIdType.MESH

epsilon = 1e-06
momentum_decay = 0.8
clip_level = 0.5
weight_decay = 0.2
step_rate = 0.1

GROUPS = 8
CHUNK = ((0, 1), (2, 3), (0, 2), (1, 3), (2, 0), (3, 1), (0, 2), (1, 3))
NT = (((1,), (1,)), ((), ()))


def dot(left, right, dims=(((1,), (0,)), ((), ()))):
    return lax.dot_general(left, right, dims, preferred_element_type=jnp.float32)


def kernel(
    entries,
    q1, k1, q2, k2, val, mix, gain, cot, left, right, weight, momentum,
    step_out, weight_out, momentum_out, copy_out,
    cm, cp, at_own, at_send, at_part, gsend, rs1, s1b, rs2, gall, wall, ssx, ssb, ssa, ssd,
    x_s, x_r, c_s, c_r, a_s, a_r, r1_s, r1_r, r2_s, r2_r,
    gb_s, gb_r, ga_s, ga_r, gd_s, gd_r, wb_s, wb_r, wa_s, wa_r, wd_s, wd_r,
    sx_s, sx_r, sb_s, sb_r, sa_s, sa_r, sd_s, sd_r,
):
    z, y, c, x = (lax.axis_index(name) for name in (*FS, "tp"))
    n = rs2.shape[0]
    nx = ssx.shape[0]
    other = 1 - c
    a = z * other + y * c
    b = y * other + z * c

    def at_a(p):
        return (p * other + z * c, y * other + p * c, c, x)

    def at_b(p):
        return (z * other + p * c, p * other + y * c, c, x)

    def at_x(p):
        return (z, y, c, p)

    partner = (z, y, other, x)
    pending = []

    def remote(src, dst, send, recv, where):
        return pltpu.make_async_remote_copy(
            src_ref=src, dst_ref=dst, send_sem=send, recv_sem=recv,
            device_id=where, device_id_type=MESH_ID,
        )

    def start(*parts):
        copy = remote(*parts)
        copy.start()
        pending.append(copy)

    def arrived(dst, send, recv):
        remote(dst, dst, send, recv, partner).wait_recv()

    def around(p, size):
        return lax.rem(p + size, size)

    barrier = pltpu.get_barrier_semaphore()
    peers = [partner]
    for d in range(1, n):
        peers += [at_a(around(a + d, n)), at_b(around(b + d, n))]
    for d in range(1, nx):
        peers.append(at_x(around(x + d, nx)))
    for peer in peers:
        pl.semaphore_signal(barrier, inc=1, device_id=peer, device_id_type=MESH_ID)
    pl.semaphore_wait(barrier, len(peers))

    tokens = cot.shape[0]
    ch = cot.shape[1] // 4
    ahead = at_x(around(x + 1, nx))
    behind = at_x(around(x - 1, nx))

    def half(i):
        return pl.ds(i * ch, ch)

    for g in range(2, 6):
        for i, where in ((0, ahead), (1, behind)):
            start(cot.at[:, half(CHUNK[g][i])], cm.at[g - 2, :, half(i)],
                  x_s.at[g - 2, i], x_r.at[g - 2, i], where)
    for g in range(2):
        start(cot.at[:, pl.ds(2 * g * ch, 2 * ch)], cp.at[g], c_s.at[g], c_r.at[g], partner)

    key_width = q1.shape[1] // 2
    value_width = val.shape[1] // 2
    block = tokens // 5

    def attend(h, out):
        ratio = mix[h]
        keyed = pl.ds(pl.multiple_of(h * key_width, key_width), key_width)
        valued = pl.ds(pl.multiple_of(h * value_width, value_width), value_width)
        for at in range(5):
            low, high = at * block, (at + 1) * block
            rows = lax.broadcasted_iota(jnp.int32, (block, high), 0) + low
            seen = lax.broadcasted_iota(jnp.int32, (block, high), 1) <= rows

            def probs(query, keys):
                scores = dot(query[low:high, keyed], keys[0:high, keyed], NT) * key_width ** (-0.5)
                scores = jnp.where(seen, scores, -jnp.inf)
                grown = jnp.exp(scores - jnp.max(scores, axis=1, keepdims=True))
                return grown, 1.0 / jnp.sum(grown, axis=1, keepdims=True)

            one, one_scale = probs(q1, k1)
            two, two_scale = probs(q2, k2)
            mixed = (one * one_scale - ratio * (two * two_scale)).astype(jnp.bfloat16)
            head = dot(mixed, val[0:high, valued])
            square = jnp.mean(head * head, axis=1, keepdims=True)
            normed = head * lax.rsqrt(square + epsilon) * gain[...]
            out[:, low:high] = normed.T.astype(jnp.bfloat16)

    def take(g):
        for i in range(2):
            arrived(cm.at[g - 2, :, half(i)], x_s.at[g - 2, i], x_r.at[g - 2, i])
        if g < 4:
            for i, where in ((0, ahead), (1, behind)):
                start(cm.at[g - 2, :, half(i)], cm.at[g + 2, :, half(i)],
                      x_s.at[g + 2, i], x_r.at[g + 2, i], where)
        start(cm.at[g - 2], cp.at[g], c_s.at[g], c_r.at[g], partner)

    attend(other, at_send)
    start(at_send, at_part, a_s, a_r, partner)
    take(2)
    attend(c, at_own)
    take(3)
    arrived(at_part, a_s, a_r)

    parts = gsend.shape[2]

    def summed(g):
        for d in range(1, n):
            arrived(rs1.at[g, d], r1_s.at[g, d], r1_r.at[g, d])
        total = rs1[g, 0].astype(jnp.float32)
        for d in range(1, n):
            total = total + rs1[g, d].astype(jnp.float32)
        s1b[g] = total.astype(jnp.bfloat16)

    for g in range(GROUPS):
        if g >= 4:
            take(g)
        mine = cot[:, 2 * g * ch : 2 * (g + 1) * ch] if g < 2 else cm[g - 2]
        grad = dot(at_own[...], mine)
        arrived(cp.at[g], c_s.at[g], c_r.at[g])
        grad = grad + dot(at_part[...], cp[g])
        gsend[g] = grad.reshape(n, parts, 2 * ch).astype(jnp.bfloat16)
        rs1[g, 0] = gsend[g, a]
        for d in range(1, n):
            p = around(a + d, n)
            start(gsend.at[g, p], rs1.at[g, d], r1_s.at[g, d], r1_r.at[g, d], at_a(p))
        if g >= 2:
            summed(g - 2)
    for g in range(GROUPS - 2, GROUPS):
        summed(g)

    per = GROUPS // n
    for d in range(1, n):
        p = around(b + d, n)
        start(s1b.at[pl.ds(p * per, per)], rs2.at[d], r2_s.at[d], r2_r.at[d], at_b(p))
    total = s1b[pl.ds(b * per, per)].astype(jnp.float32)
    for d in range(1, n):
        arrived(rs2.at[d], r2_s.at[d], r2_r.at[d])
        total = total + rs2[d].astype(jnp.float32)
    gall[c, a, pl.ds(b * per, per)] = total.astype(jnp.bfloat16)

    def gather(buf, count, b_s, b_r, a_s, a_r, d_s, d_r):
        own = buf.at[c, a, pl.ds(b * count, count)]
        for d in range(1, n):
            start(own, own, b_s.at[d], b_r.at[d], at_b(around(b + d, n)))
        for d in range(1, n):
            arrived(buf.at[c, a, pl.ds(around(b - d, n) * count, count)], b_s.at[d], b_r.at[d])
        line = buf.at[c, a]
        for d in range(1, n):
            start(line, line, a_s.at[d], a_r.at[d], at_a(around(a + d, n)))
        start(line, line, d_s.at[0], d_r.at[0], partner)
        for d in range(1, n):
            line = buf.at[c, around(a - d, n)]
            arrived(line, a_s.at[d], a_r.at[d])
            start(line, line, d_s.at[d], d_r.at[d], partner)
        for d in range(n):
            arrived(buf.at[other, around(b - d, n)], d_s.at[d], d_r.at[d])

    gather(gall, per, gb_s, gb_r, ga_s, ga_r, gd_s, gd_r)

    sources = (x, x, None, None, None, None, around(x + 2, nx), around(x + 2, nx))
    sides = (around(x - 1, nx), around(x + 1, nx))
    left_done = jnp.zeros(momentum.shape, jnp.float32)
    for g in range(GROUPS):
        columns = []
        for i in range(2):
            source = sides[i] if sources[g] is None else sources[g]
            at = pl.multiple_of((source * 4 + CHUNK[g][i]) * ch, ch)
            columns.append(left[:, pl.ds(at, ch)])
        grown = gall[:, :, g].reshape(2 * value_width, 2 * ch)
        left_done = left_done + dot(jnp.concatenate(columns, axis=1), grown, NT)

    high = left_done.astype(jnp.bfloat16)
    rest = left_done - high.astype(jnp.float32)
    middle = rest.astype(jnp.bfloat16)
    low = (rest - middle.astype(jnp.float32)).astype(jnp.bfloat16)
    done = []
    for h in range(2):
        columns = slice(h * value_width, (h + 1) * value_width)
        root = right[columns, :]
        done.append(dot(high[:, columns], root) + (dot(middle[:, columns], root) + dot(low[:, columns], root)))
    preconditioned = jnp.concatenate(done, axis=1)
    fresh = momentum_decay * momentum[...] + (1.0 - momentum_decay) * preconditioned
    momentum_out[...] = fresh

    def exchanged(value, slots, send, recv, where, at, size):
        slots[0] = value
        for d in range(1, size):
            start(slots.at[0], slots.at[d], send.at[d], recv.at[d], where(around(at + d, size)))
        for d in range(1, size):
            arrived(slots.at[d], send.at[d], recv.at[d])
            value = value + slots[d]
        return value

    squares = jnp.broadcast_to(jnp.sum(fresh * fresh, keepdims=True), ssx.shape[1:])
    squares = exchanged(squares, ssx, sx_s, sx_r, at_x, x, nx)
    squares = exchanged(squares, ssb, sb_s, sb_r, at_b, b, n)
    squares = exchanged(squares, ssa, sa_s, sa_r, at_a, a, n)
    squares = exchanged(squares, ssd, sd_s, sd_r, lambda p: partner, c, 2)
    factor = clip_level * lax.rsqrt(squares[0:1, 0:1] / entries + epsilon)
    step = factor * fresh + weight_decay * weight[...]
    step_out[...] = step
    new = weight[...] - step_rate * step
    weight_out[...] = new
    wall[c, a, b] = new.astype(jnp.bfloat16)
    gather(wall, 1, wb_s, wb_r, wa_s, wa_r, wd_s, wd_r)

    def laid(i, carry):
        copy_out[i, :, 0] = wall[0, i]
        copy_out[:, i, 1] = wall[1, i]
        return carry

    lax.fori_loop(0, n, laid, 0)
    for copy in pending:
        copy.wait_send()


def local(
    query_one, key_one, query_two, key_two, values, mix_ratio, head_gain,
    cotangent, left_roots, right_roots, weight, momentum,
):
    n = lax.axis_size("fs_0")
    nx = lax.axis_size("tp")
    tokens, own_cols = cotangent.shape
    rows = weight.shape[0]
    width = values.shape[1] // 2
    parts = width // n
    pair = own_cols // 2
    bf16, f32 = jnp.bfloat16, jnp.float32
    dma = pltpu.SemaphoreType.DMA
    vmem = pl.BlockSpec(memory_space=pltpu.VMEM)
    smem = pl.BlockSpec(memory_space=pltpu.SMEM)
    tile = (8, 128)
    shapes = pltpu.VMEM
    scratch = [
        shapes((GROUPS - 2, tokens, pair), bf16),
        shapes((GROUPS, tokens, pair), bf16),
        shapes((width, tokens), bf16),
        shapes((width, tokens), bf16),
        shapes((width, tokens), bf16),
        shapes((GROUPS, n, parts, pair), bf16),
        shapes((GROUPS, n, parts, pair), bf16),
        shapes((GROUPS, parts, pair), bf16),
        shapes((n, GROUPS // n, parts, pair), bf16),
        shapes((2, n, GROUPS, parts, pair), bf16),
        shapes((2, n, n, rows, own_cols), bf16),
        shapes((nx, *tile), f32),
        shapes((n, *tile), f32),
        shapes((n, *tile), f32),
        shapes((2, *tile), f32),
    ]
    for shape in ((GROUPS - 2, 2), (GROUPS,), (), (GROUPS, n), (n,), (n,), (n,), (n,), (n,), (n,), (n,), (nx,), (n,), (n,), (2,)):
        scratch += [dma(shape) if shape else dma] * 2
    step, weight_new, momentum_new, copied = pl.pallas_call(
        functools.partial(kernel, float(weight.size * n * n * 2 * nx)),
        out_shape=(
            jax.ShapeDtypeStruct(weight.shape, f32),
            jax.ShapeDtypeStruct(weight.shape, f32),
            jax.ShapeDtypeStruct(weight.shape, f32),
            jax.ShapeDtypeStruct((n, n, 2, rows, own_cols), bf16),
        ),
        in_specs=[vmem] * 5 + [smem] + [vmem] * 6,
        out_specs=[vmem] * 4,
        scratch_shapes=scratch,
        compiler_params=pltpu.CompilerParams(
            collective_id=0, has_side_effects=True, vmem_limit_bytes=60 * 1024 * 1024
        ),
    )(
        query_one, key_one, query_two, key_two, values, mix_ratio, head_gain.reshape(1, -1),
        cotangent, left_roots, right_roots, weight, momentum,
    )
    return step, weight_new, momentum_new, copied.reshape(-1, own_cols)


def split_mesh(mesh):
    lines = int((mesh.shape["fs"] // 2) ** 0.5)
    return Mesh(mesh.devices.reshape(lines, lines, 2, mesh.shape["tp"]), (*FS, "tp"))


def solution(mesh):
    return jax.shard_map(
        local,
        mesh=split_mesh(mesh),
        in_specs=(
            P(FS, "tp"), P(FS, "tp"), P(FS, "tp"), P(FS, "tp"), P(FS, "tp"), P("tp"), P(),
            P(FS, "tp"), P(FS, None), P("tp", None), P(FS, "tp"), P(FS, "tp"),
        ),
        out_specs=(P(FS, "tp"), P(FS, "tp"), P(FS, "tp"), P(None, "tp")),
        check_vma=False,
    )
```

```python
import functools

import jax
import jax.numpy as jnp
from jax import lax
from jax.experimental import pallas as pl
from jax.experimental.pallas import tpu as pltpu
from jax.sharding import Mesh
from jax.sharding import PartitionSpec as P

FS = ("fs_0", "fs_1", "fs_2")
MESH_ID = pl.DeviceIdType.MESH

epsilon = 1e-06
momentum_decay = 0.8
clip_level = 0.5
weight_decay = 0.2
step_rate = 0.1

GROUPS = 8
CHUNK = ((0, 1), (2, 3), (0, 2), (1, 3), (2, 0), (3, 1), (0, 2), (1, 3))
NT = (((1,), (1,)), ((), ()))


def dot(left, right, dims=(((1,), (0,)), ((), ()))):
    return lax.dot_general(left, right, dims, preferred_element_type=jnp.float32)


def kernel(
    entries,
    q1_in, k1_in, q2_in, k2_in, val_in, mix_in, gain_in, cot_in, left_in, right_in, weight_in, momentum_in,
    grown_out, factor_out, copy_out,
    q1, k1, q2, k2, val, mix, gain, cot, right, load,
    cm, cp, at_own, at_send, at_part, gsend, rs1, s1b, rs2, gall, wall, mall, ssx, ssa, ssd,
    left, momentum, grown_line,
    x_s, x_r, c_s, c_r, a_s, a_r, r1_s, r1_r, r2_s, r2_r,
    gb_s, gb_r, ga_s, ga_r, gd_s, gd_r, ma_s, ma_r, md_s, md_r,
    wb_s, wb_r, wa_s, wa_r, wd_s, wd_r, lb_s, lb_r, pb_s, pb_r,
    sx_s, sx_r, sa_s, sa_r, sd_s, sd_r,
):
    z, y, c, x = (lax.axis_index(name) for name in (*FS, "tp"))
    n = rs2.shape[0]
    nx = ssx.shape[0]
    other = 1 - c
    a = z * other + y * c
    b = y * other + z * c

    def at_a(p):
        return (p * other + z * c, y * other + p * c, c, x)

    def at_b(p):
        return (z * other + p * c, p * other + y * c, c, x)

    def at_x(p):
        return (z, y, c, p)

    partner = (z, y, other, x)

    def remote(src, dst, send, recv, where):
        return pltpu.make_async_remote_copy(
            src_ref=src, dst_ref=dst, send_sem=send, recv_sem=recv,
            device_id=where, device_id_type=MESH_ID,
        )

    def start(*parts):
        remote(*parts).start()

    def arrived(dst, send, recv):
        remote(dst, dst, send, recv, partner).wait_recv()

    def sent(src, send, recv):
        remote(src, src, send, recv, partner).wait_send()

    def around(p, size):
        return lax.rem(p + size, size)

    loads = {}
    for i, (name, src, dst) in enumerate((
        ("cot", cot_in, cot), ("q1", q1_in, q1), ("k1", k1_in, k1), ("q2", q2_in, q2), ("k2", k2_in, k2),
        ("val", val_in, val), ("gain", gain_in, gain), ("mix", mix_in, mix), ("weight", weight_in, wall.at[c, a, b]),
        ("left", left_in, left.at[b]), ("right", right_in, right), ("momentum", momentum_in, momentum.at[b]),
    )):
        loads[name] = pltpu.make_async_copy(src, dst, load.at[i])
        loads[name].start()

    barrier = pltpu.get_barrier_semaphore()
    peers = [partner]
    for d in range(1, n):
        peers += [at_a(around(a + d, n)), at_b(around(b + d, n))]
    for d in range(1, nx):
        peers.append(at_x(around(x + d, nx)))
    for peer in peers:
        pl.semaphore_signal(barrier, inc=1, device_id=peer, device_id_type=MESH_ID)
    pl.semaphore_wait(barrier, len(peers))

    tokens = cot.shape[0]
    ch = cot.shape[1] // 4
    ahead = at_x(around(x + 1, nx))
    behind = at_x(around(x - 1, nx))

    def half(i):
        return pl.ds(i * ch, ch)

    loads["cot"].wait()
    for g in range(2, 6):
        for i, where in ((0, ahead), (1, behind)):
            start(cot.at[:, half(CHUNK[g][i])], cm.at[g - 2, :, half(i)], x_s, x_r.at[g - 2], where)
    for g in range(2):
        start(cot.at[:, pl.ds(2 * g * ch, 2 * ch)], cp.at[g], c_s, c_r.at[g], partner)
    for name, held, send, recv in (
        ("weight", wall.at[c, a, b], wb_s, wb_r), ("momentum", momentum.at[b], pb_s, pb_r), ("left", left.at[b], lb_s, lb_r),
    ):
        loads[name].wait()
        for d in range(1, n):
            start(held, held, send, recv, at_b(around(b + d, n)))

    for name in ("q1", "k1", "q2", "k2", "val", "gain", "mix"):
        loads[name].wait()
    key_width = q1.shape[1] // 2
    value_width = val.shape[1] // 2
    block = tokens // 5

    def attend(h, out):
        chosen = lax.broadcasted_iota(jnp.int32, (1, 2), 1) == h
        ratio = jnp.sum(jnp.where(chosen, mix[...], 0.0), axis=1, keepdims=True)
        keyed = pl.ds(pl.multiple_of(h * key_width, key_width), key_width)
        valued = pl.ds(pl.multiple_of(h * value_width, value_width), value_width)
        for at in range(5):
            low, high = at * block, (at + 1) * block
            rows = lax.broadcasted_iota(jnp.int32, (block, high), 0) + low
            seen = lax.broadcasted_iota(jnp.int32, (block, high), 1) <= rows

            def probs(query, keys):
                scores = dot(query[low:high, keyed], keys[0:high, keyed], NT) * key_width ** (-0.5)
                scores = jnp.where(seen, scores, -jnp.inf)
                grown = jnp.exp(scores - jnp.max(scores, axis=1, keepdims=True))
                return grown, 1.0 / jnp.sum(grown, axis=1, keepdims=True)

            one, one_scale = probs(q1, k1)
            two, two_scale = probs(q2, k2)
            mixed = (one * one_scale - ratio * (two * two_scale)).astype(jnp.bfloat16)
            head = dot(mixed, val[0:high, valued])
            square = jnp.mean(head * head, axis=1, keepdims=True)
            normed = head * lax.rsqrt(square + epsilon) * gain[...]
            out[:, low:high] = normed.T.astype(jnp.bfloat16)

    def take(g):
        arrived(cm.at[g - 2], x_s, x_r.at[g - 2])
        if g < 4:
            for i, where in ((0, ahead), (1, behind)):
                start(cm.at[g - 2, :, half(i)], cm.at[g + 2, :, half(i)], x_s, x_r.at[g + 2], where)
        start(cm.at[g - 2], cp.at[g], c_s, c_r.at[g], partner)

    up = n // 2
    steps = [(h, 1, h == up) for h in range(1, up + 1)] + [(h, -1, h == n - 1 - up) for h in range(1, n - up)]

    def line_of(index, home):
        h, way, _ = steps[index]
        return around(home - way * h, n)

    def weight_lines(h):
        for index, (hop, way, last) in enumerate(steps):
            if hop != h:
                continue
            line = wall.at[c, line_of(index, a)]
            arrived(line, wa_s, wa_r.at[index])
            if not last:
                start(line, line, wa_s, wa_r.at[index + 1], at_a(around(a + way, n)))
            start(line, line, wd_s, wd_r, partner)

    attend(other, at_send)
    start(at_send, at_part, a_s, a_r, partner)
    take(2)
    arrived(wall.at[c, a, pl.ds(0, n - 1)], wb_s, wb_r)
    line = wall.at[c, a]
    for index, (h, way, _) in enumerate(steps):
        if h == 1:
            start(line, line, wa_s, wa_r.at[index], at_a(around(a + way, n)))
    start(line, line, wd_s, wd_r, partner)
    attend(c, at_own)
    take(3)
    arrived(at_part, a_s, a_r)

    parts = gsend.shape[2]
    others = pl.ds(1, n - 1)

    def summed(g):
        arrived(rs1.at[g, others], r1_s, r1_r.at[g])
        total = rs1[g, 0].astype(jnp.float32)
        for d in range(1, n):
            total = total + rs1[g, d].astype(jnp.float32)
        s1b[g] = total.astype(jnp.bfloat16)

    for g in range(GROUPS):
        if g >= 4:
            take(g)
        mine = cot[:, 2 * g * ch : 2 * (g + 1) * ch] if g < 2 else cm[g - 2]
        grad = dot(at_own[...], mine)
        arrived(cp.at[g], c_s, c_r.at[g])
        grad = grad + dot(at_part[...], cp[g])
        gsend[g] = grad.reshape(n, parts, 2 * ch).astype(jnp.bfloat16)
        rs1[g, 0] = gsend[g, a]
        for d in range(1, n):
            p = around(a + d, n)
            start(gsend.at[g, p], rs1.at[g, d], r1_s, r1_r.at[g], at_a(p))
        if g == 5:
            weight_lines(1)
        if g >= 5:
            summed(g - 5)
    weight_lines(2)
    sent(cm, x_s, x_r.at[0])
    sent(cp, c_s, c_r.at[0])
    sent(at_send, a_s, a_r)
    for g in range(GROUPS - 5, GROUPS):
        summed(g)

    per = GROUPS // n
    for d in range(1, n):
        p = around(b + d, n)
        start(s1b.at[pl.ds(p * per, per)], rs2.at[d], r2_s, r2_r, at_b(p))
    sent(rs1.at[:, others], r1_s, r1_r.at[0])
    sent(wall.at[c, a, pl.ds(0, n - 1)], wb_s, wb_r)
    for held, send, recv in ((momentum, pb_s, pb_r), (left, lb_s, lb_r)):
        sent(held.at[pl.ds(0, n - 1)], send, recv)
        arrived(held.at[pl.ds(0, n - 1)], send, recv)
    loads["right"].wait()
    total = s1b[pl.ds(b * per, per)].astype(jnp.float32)
    arrived(rs2.at[others], r2_s, r2_r)
    for d in range(1, n):
        total = total + rs2[d].astype(jnp.float32)
    gall[c, a, pl.ds(b * per, per)] = total.astype(jnp.bfloat16)

    own = gall.at[c, a, pl.ds(b * per, per)]
    for d in range(1, n):
        start(own, own, gb_s, gb_r, at_b(around(b + d, n)))
    sent(rs2.at[others], r2_s, r2_r)
    arrived(gall.at[c, a, pl.ds(0, (n - 1) * per)], gb_s, gb_r)

    def ring(buf, a_s, a_r, d_s, d_r, extra):
        pieces = a_r.shape[1]
        count = buf.shape[2] // pieces
        waiting = [pieces] * len(steps)

        def piece(line, k):
            return buf.at[c, line, pl.ds(k * count, count)]

        def step(index, k):
            _, way, last = steps[index]
            line = line_of(index, a)
            arrived(piece(line, k), a_s, a_r.at[index, k])
            if not last:
                start(piece(line, k), piece(line, k), a_s, a_r.at[index + 1, k], at_a(around(a + way, n)))
            waiting[index] -= 1
            if waiting[index] == 0:
                start(buf.at[c, line], buf.at[c, line], d_s, d_r, partner)

        for k in range(pieces):
            for index, (h, way, _) in enumerate(steps):
                if h == 1:
                    start(piece(a, k), piece(a, k), a_s, a_r.at[index, k], at_a(around(a + way, n)))
        start(buf.at[c, a], buf.at[c, a], d_s, d_r, partner)
        events = list(extra)
        for index, (h, _, _) in enumerate(steps):
            for k in range(pieces):
                events.append((2.05 * h + 0.35 * k, functools.partial(step, index, k)))
        for order, (_, event) in enumerate(sorted(events, key=lambda pair: pair[0])):
            event()

    def drained(buf, a_s, a_r, d_s, d_r):
        sent(buf.at[c, pl.ds(0, n - 1)], a_s, a_r)
        sent(buf.at[c], d_s, d_r)

    ring(gall, ga_s, ga_r, gd_s, gd_r, ())
    sent(gall.at[c, a, pl.ds(0, (n - 1) * per)], gb_s, gb_r)
    arrived(gall.at[other], gd_s, gd_r)
    weight_lines(3)

    sources = (x, x, None, None, None, None, around(x + 2, nx), around(x + 2, nx))
    sides = (around(x - 1, nx), around(x + 1, nx))
    rows = left.shape[1]
    left_done = jnp.zeros((n * rows, 2 * value_width), jnp.float32)
    for g in range(GROUPS):
        columns = []
        for i in range(2):
            source = sides[i] if sources[g] is None else sources[g]
            at = pl.multiple_of((source * 4 + CHUNK[g][i]) * ch, ch)
            columns.append(left[:, :, pl.ds(at, ch)].reshape(n * rows, ch))
        grown = gall[:, :, g].reshape(2 * value_width, 2 * ch)
        left_done = left_done + dot(jnp.concatenate(columns, axis=1), grown, NT)

    high = left_done.astype(jnp.bfloat16)
    rest = left_done - high.astype(jnp.float32)
    middle = rest.astype(jnp.bfloat16)
    low = (rest - middle.astype(jnp.float32)).astype(jnp.bfloat16)
    done = []
    for h in range(2):
        columns = slice(h * value_width, (h + 1) * value_width)
        root = right[columns, :]
        done.append(dot(high[:, columns], root) + (dot(middle[:, columns], root) + dot(low[:, columns], root)))
    preconditioned = jnp.concatenate(done, axis=1)
    grown_line[...] = preconditioned.reshape(grown_line.shape)
    fresh = momentum_decay * momentum[...] + (1.0 - momentum_decay) * preconditioned.reshape(grown_line.shape)
    mall[c, a] = fresh.astype(jnp.bfloat16)

    def offered(value, slots, send, recv, where, at, size):
        slots[at] = value
        for d in range(1, size):
            start(slots.at[at], slots.at[at], send, recv, where(around(at + d, size)))

    stages = (
        (ssx, sx_s, sx_r, at_x, x, nx), (ssa, sa_s, sa_r, at_a, a, n), (ssd, sd_s, sd_r, lambda p: partner, c, 2),
    )
    squares = jnp.sum(jnp.sum(fresh * fresh, axis=0), keepdims=True)
    offered(jnp.broadcast_to(squares, ssx.shape[1:]), *stages[0])
    total = []

    def pass_on(index):
        slots, send, recv, _, _, size = stages[index]
        arrived(slots.at[pl.ds(0, size - 1)], send, recv)
        squares = jnp.sum(slots[...], axis=0)
        if index + 1 < len(stages):
            offered(squares, *stages[index + 1])
        else:
            total.append(squares)

    ring(mall, ma_s, ma_r, md_s, md_r,
         [(when, functools.partial(pass_on, index)) for index, when in enumerate((2.8, 7.3, 8.3))])
    factor = clip_level * lax.rsqrt(total[0] / entries + epsilon)
    factor_out[...] = factor
    grown_out[...] = grown_line[b]
    weight_lines(4)
    arrived(wall.at[other], wd_s, wd_r)
    scale = factor[0:1, 0:1].reshape(1, 1, 1)

    def final(core, line):
        held = wall[core, line]
        step = scale * mall[core, line].astype(jnp.float32) + weight_decay * held
        return (held - step_rate * step).astype(jnp.bfloat16)

    arrived(mall.at[other], md_s, md_r)

    def laid(i, carry):
        copy_out[i, :, 0] = final(0, i)
        copy_out[:, i, 1] = final(1, i)
        return carry

    lax.fori_loop(0, n, laid, 0)
    drained(gall, ga_s, ga_r.at[0, 0], gd_s, gd_r)
    drained(mall, ma_s, ma_r.at[0, 0], md_s, md_r)
    drained(wall, wa_s, wa_r.at[0], wd_s, wd_r)
    for slots, send, recv, _, _, size in stages:
        sent(slots.at[pl.ds(0, size - 1)], send, recv)


def local(
    query_one, key_one, query_two, key_two, values, mix_ratio, head_gain,
    cotangent, left_roots, right_roots, weight, momentum,
):
    n = lax.axis_size("fs_0")
    nx = lax.axis_size("tp")
    tokens, own_cols = cotangent.shape
    rows = weight.shape[0]
    width = values.shape[1] // 2
    parts = width // n
    pair = own_cols // 2
    bf16, f32 = jnp.bfloat16, jnp.float32
    dma = pltpu.SemaphoreType.DMA
    vmem = pl.BlockSpec(memory_space=pltpu.VMEM)
    hbm = pl.BlockSpec(memory_space=pltpu.HBM)
    tile = (8, 128)
    shapes = pltpu.VMEM
    gain, mix = head_gain.reshape(1, -1), mix_ratio.reshape(1, -1)
    scratch = [
        shapes(array.shape, array.dtype)
        for array in (query_one, key_one, query_two, key_two, values, mix, gain, cotangent, right_roots)
    ]
    scratch += [
        dma((12,)),
        shapes((GROUPS - 2, tokens, pair), bf16),
        shapes((GROUPS, tokens, pair), bf16),
        shapes((width, tokens), bf16),
        shapes((width, tokens), bf16),
        shapes((width, tokens), bf16),
        shapes((GROUPS, n, parts, pair), bf16),
        shapes((GROUPS, n, parts, pair), bf16),
        shapes((GROUPS, parts, pair), bf16),
        shapes((n, GROUPS // n, parts, pair), bf16),
        shapes((2, n, GROUPS, parts, pair), bf16),
        shapes((2, n, n, rows, own_cols), f32),
        shapes((2, n, n, rows, own_cols), bf16),
        shapes((nx, *tile), f32),
        shapes((n, *tile), f32),
        shapes((2, *tile), f32),
        shapes((n, *left_roots.shape), bf16),
        shapes((n, rows, own_cols), f32),
        shapes((n, rows, own_cols), f32),
    ]
    pieces = min(4, n)
    for received in (
        (GROUPS - 2,), (GROUPS,), (), (GROUPS,), (), (), (n - 1, pieces), (), (n - 1, pieces), (),
        (), (n - 1,), (), (), (), (), (), (),
    ):
        scratch += [dma, dma(received) if received else dma]
    inputs = [
        pltpu.with_memory_space_constraint(array, pltpu.HBM)
        for array in (
            query_one, key_one, query_two, key_two, values, mix, gain,
            cotangent, left_roots, right_roots, weight, momentum,
        )
    ]
    grown, factor, copied = pl.pallas_call(
        functools.partial(kernel, float(weight.size * n * n * 2 * nx)),
        out_shape=(
            jax.ShapeDtypeStruct(weight.shape, f32),
            jax.ShapeDtypeStruct(tile, f32),
            jax.ShapeDtypeStruct((n, n, 2, rows, own_cols), bf16),
        ),
        in_specs=[hbm] * 12,
        out_specs=[vmem] * 3,
        scratch_shapes=scratch,
        compiler_params=pltpu.CompilerParams(
            collective_id=0, has_side_effects=True, vmem_limit_bytes=40 * 1024 * 1024
        ),
    )(*inputs)
    momentum_new = momentum_decay * momentum + (1.0 - momentum_decay) * grown
    step = factor[0, 0] * momentum_new + weight_decay * weight
    weight_new = weight - step_rate * step
    return step, weight_new, momentum_new, copied.reshape(-1, own_cols)


def split_mesh(mesh):
    lines = int((mesh.shape["fs"] // 2) ** 0.5)
    return Mesh(mesh.devices.reshape(lines, lines, 2, mesh.shape["tp"]), (*FS, "tp"))


def solution(mesh):
    return jax.shard_map(
        local,
        mesh=split_mesh(mesh),
        in_specs=(
            P(FS, "tp"), P(FS, "tp"), P(FS, "tp"), P(FS, "tp"), P(FS, "tp"), P("tp"), P(),
            P(FS, "tp"), P(FS, None), P("tp", None), P(FS, "tp"), P(FS, "tp"),
        ),
        out_specs=(P(FS, "tp"), P(FS, "tp"), P(FS, "tp"), P(None, "tp")),
        check_vma=False,
    )
```

```python
import functools

import jax
import jax.numpy as jnp
from jax import lax
from jax.experimental import pallas as pl
from jax.experimental.pallas import tpu as pltpu
from jax.sharding import Mesh
from jax.sharding import PartitionSpec as P

FS = ("fs_0", "fs_1", "fs_2")
MESH_ID = pl.DeviceIdType.MESH

epsilon = 1e-06
momentum_decay = 0.8
clip_level = 0.5
weight_decay = 0.2
step_rate = 0.1

GROUPS = 8
CHUNK = ((0, 1), (2, 3), (0, 2), (1, 3), (2, 0), (3, 1), (0, 2), (1, 3))
NT = (((1,), (1,)), ((), ()))


def dot(left, right, dims=(((1,), (0,)), ((), ()))):
    return lax.dot_general(left, right, dims, preferred_element_type=jnp.float32)


def kernel(
    entries,
    q1_in, k1_in, q2_in, k2_in, val_in, mix_in, gain_in, cot_in, left_in, right_in, weight_in, momentum_in,
    grown_out, factor_out, copy_out,
    q1, k1, q2, k2, val, mix, gain, cot, right, load,
    cm, cp, at_own, at_send, at_part, gsend, rs1, s1b, rs2, gall, wall, mall, ssx, ssa, ssd,
    left, momentum, grown_line,
    x_s, x_r, c_s, c_r, a_s, a_r, r1_s, r1_r, r2_s, r2_r,
    gb_s, gb_r, ga_s, ga_r, gd_s, gd_r, ma_s, ma_r, md_s, md_r,
    wb_s, wb_r, wa_s, wa_r, wd_s, wd_r, lb_s, lb_r, pb_s, pb_r,
    sx_s, sx_r, sa_s, sa_r, sd_s, sd_r,
):
    z, y, c, x = (lax.axis_index(name) for name in (*FS, "tp"))
    n = rs2.shape[0]
    nx = ssx.shape[0]
    other = 1 - c
    a = z * other + y * c
    b = y * other + z * c

    def at_a(p):
        return (p * other + z * c, y * other + p * c, c, x)

    def at_b(p):
        return (z * other + p * c, p * other + y * c, c, x)

    def at_x(p):
        return (z, y, c, p)

    partner = (z, y, other, x)

    def remote(src, dst, send, recv, where):
        return pltpu.make_async_remote_copy(
            src_ref=src, dst_ref=dst, send_sem=send, recv_sem=recv,
            device_id=where, device_id_type=MESH_ID,
        )

    def start(*parts):
        remote(*parts).start()

    def arrived(dst, send, recv):
        remote(dst, dst, send, recv, partner).wait_recv()

    def sent(src, send, recv):
        remote(src, src, send, recv, partner).wait_send()

    def around(p, size):
        return lax.rem(p + size, size)

    loads = {}
    for i, (name, src, dst) in enumerate((
        ("cot", cot_in, cot), ("q1", q1_in, q1), ("k1", k1_in, k1), ("q2", q2_in, q2), ("k2", k2_in, k2),
        ("val", val_in, val), ("gain", gain_in, gain), ("mix", mix_in, mix), ("weight", weight_in, wall.at[c, a, b]),
        ("left", left_in, left.at[b]), ("right", right_in, right), ("momentum", momentum_in, momentum.at[b]),
    )):
        loads[name] = pltpu.make_async_copy(src, dst, load.at[i])
        loads[name].start()

    barrier = pltpu.get_barrier_semaphore()
    peers = [partner]
    for d in range(1, n):
        peers += [at_a(around(a + d, n)), at_b(around(b + d, n))]
    for d in range(1, nx):
        peers.append(at_x(around(x + d, nx)))
    for peer in peers:
        pl.semaphore_signal(barrier, inc=1, device_id=peer, device_id_type=MESH_ID)
    pl.semaphore_wait(barrier, len(peers))

    tokens = cot.shape[0]
    ch = cot.shape[1] // 4
    ahead = at_x(around(x + 1, nx))
    behind = at_x(around(x - 1, nx))

    def half(i):
        return pl.ds(i * ch, ch)

    loads["cot"].wait()
    for g in range(2, 6):
        for i, where in ((0, ahead), (1, behind)):
            start(cot.at[:, half(CHUNK[g][i])], cm.at[g - 2, :, half(i)], x_s, x_r.at[g - 2], where)
    for g in range(2):
        start(cot.at[:, pl.ds(2 * g * ch, 2 * ch)], cp.at[g], c_s, c_r.at[g], partner)
    for name, held, send, recv in (
        ("weight", wall.at[c, a, b], wb_s, wb_r), ("momentum", momentum.at[b], pb_s, pb_r), ("left", left.at[b], lb_s, lb_r),
    ):
        loads[name].wait()
        for d in range(1, n):
            start(held, held, send, recv, at_b(around(b + d, n)))

    for name in ("q1", "k1", "q2", "k2", "val", "gain", "mix"):
        loads[name].wait()
    key_width = q1.shape[1] // 2
    value_width = val.shape[1] // 2
    block = tokens // 5

    def attend(h, out):
        chosen = lax.broadcasted_iota(jnp.int32, (1, 2), 1) == h
        ratio = jnp.sum(jnp.where(chosen, mix[...], 0.0), axis=1, keepdims=True)
        keyed = pl.ds(pl.multiple_of(h * key_width, key_width), key_width)
        valued = pl.ds(pl.multiple_of(h * value_width, value_width), value_width)
        for at in range(5):
            low, high = at * block, (at + 1) * block
            rows = lax.broadcasted_iota(jnp.int32, (block, high), 0) + low
            seen = lax.broadcasted_iota(jnp.int32, (block, high), 1) <= rows

            def probs(query, keys):
                scores = dot(query[low:high, keyed], keys[0:high, keyed], NT) * key_width ** (-0.5)
                scores = jnp.where(seen, scores, -jnp.inf)
                grown = jnp.exp(scores - jnp.max(scores, axis=1, keepdims=True))
                return grown, 1.0 / jnp.sum(grown, axis=1, keepdims=True)

            one, one_scale = probs(q1, k1)
            two, two_scale = probs(q2, k2)
            mixed = (one * one_scale - ratio * (two * two_scale)).astype(jnp.bfloat16)
            head = dot(mixed, val[0:high, valued])
            square = jnp.mean(head * head, axis=1, keepdims=True)
            normed = head * lax.rsqrt(square + epsilon) * gain[...]
            out[:, low:high] = normed.T.astype(jnp.bfloat16)

    def take(g):
        arrived(cm.at[g - 2], x_s, x_r.at[g - 2])
        if g < 4:
            for i, where in ((0, ahead), (1, behind)):
                start(cm.at[g - 2, :, half(i)], cm.at[g + 2, :, half(i)], x_s, x_r.at[g + 2], where)
        start(cm.at[g - 2], cp.at[g], c_s, c_r.at[g], partner)

    up = n // 2
    steps = [(h, 1, h == up) for h in range(1, up + 1)] + [(h, -1, h == n - 1 - up) for h in range(1, n - up)]

    def line_of(index, home):
        h, way, _ = steps[index]
        return around(home - way * h, n)

    def weight_lines(h):
        for index, (hop, way, last) in enumerate(steps):
            if hop != h:
                continue
            line = wall.at[c, line_of(index, a)]
            arrived(line, wa_s, wa_r.at[index])
            if not last:
                start(line, line, wa_s, wa_r.at[index + 1], at_a(around(a + way, n)))
            start(line, line, wd_s, wd_r, partner)

    attend(other, at_send)
    start(at_send, at_part, a_s, a_r, partner)
    take(2)
    arrived(wall.at[c, a, pl.ds(0, n - 1)], wb_s, wb_r)
    line = wall.at[c, a]
    for index, (h, way, _) in enumerate(steps):
        if h == 1:
            start(line, line, wa_s, wa_r.at[index], at_a(around(a + way, n)))
    start(line, line, wd_s, wd_r, partner)
    attend(c, at_own)
    take(3)
    arrived(at_part, a_s, a_r)

    parts = gsend.shape[2]
    others = pl.ds(1, n - 1)

    def summed(g):
        arrived(rs1.at[g, others], r1_s, r1_r.at[g])
        total = rs1[g, 0].astype(jnp.float32)
        for d in range(1, n):
            total = total + rs1[g, d].astype(jnp.float32)
        s1b[g] = total.astype(jnp.bfloat16)

    for g in range(GROUPS):
        if g >= 4:
            take(g)
        mine = cot[:, 2 * g * ch : 2 * (g + 1) * ch] if g < 2 else cm[g - 2]
        grad = dot(at_own[...], mine)
        arrived(cp.at[g], c_s, c_r.at[g])
        grad = grad + dot(at_part[...], cp[g])
        gsend[g] = grad.reshape(n, parts, 2 * ch).astype(jnp.bfloat16)
        rs1[g, 0] = gsend[g, a]
        for d in range(1, n):
            p = around(a + d, n)
            start(gsend.at[g, p], rs1.at[g, d], r1_s, r1_r.at[g], at_a(p))
        if g >= 5:
            summed(g - 5)
    weight_lines(1)
    sent(cm, x_s, x_r.at[0])
    sent(cp, c_s, c_r.at[0])
    sent(at_send, a_s, a_r)
    for g in range(GROUPS - 5, GROUPS):
        summed(g)

    per = GROUPS // n
    for d in range(1, n):
        p = around(b + d, n)
        start(s1b.at[pl.ds(p * per, per)], rs2.at[d], r2_s, r2_r, at_b(p))
    sent(rs1.at[:, others], r1_s, r1_r.at[0])
    weight_lines(2)
    sent(wall.at[c, a, pl.ds(0, n - 1)], wb_s, wb_r)
    for held, send, recv in ((momentum, pb_s, pb_r), (left, lb_s, lb_r)):
        sent(held.at[pl.ds(0, n - 1)], send, recv)
        arrived(held.at[pl.ds(0, n - 1)], send, recv)
    loads["right"].wait()
    total = s1b[pl.ds(b * per, per)].astype(jnp.float32)
    arrived(rs2.at[others], r2_s, r2_r)
    for d in range(1, n):
        total = total + rs2[d].astype(jnp.float32)
    gall[c, a, pl.ds(b * per, per)] = total.astype(jnp.bfloat16)

    own = gall.at[c, a, pl.ds(b * per, per)]
    for d in range(1, n):
        start(own, own, gb_s, gb_r, at_b(around(b + d, n)))
    sent(rs2.at[others], r2_s, r2_r)
    weight_lines(3)
    arrived(gall.at[c, a, pl.ds(0, (n - 1) * per)], gb_s, gb_r)

    down = n - 1 - up
    away = list(range(1, up + 1)) + [-d for d in range(1, down + 1)]

    def spread(buf, a_s, a_r, d_s, d_r, extra):
        pieces = a_r.shape[1]
        count = buf.shape[2] // pieces
        waiting = [pieces] * len(away)

        def send(line, k, to, index):
            part = buf.at[c, line, pl.ds(k * count, count)]
            start(part, part, a_s, a_r.at[index, k], at_a(around(a + to, n)))

        def step(s, k):
            index = away.index(s)
            line = around(a - s, n)
            arrived(buf.at[c, line, pl.ds(k * count, count)], a_s, a_r.at[index, k])
            if s == 2:
                if up > 3 and k % 2 == 0:
                    send(line, k, 2, away.index(4))
                if up > 2:
                    send(line, k, 1, away.index(3))
            if s == -2:
                if up > 3 and k % 2 == 1:
                    send(line, k, -2, away.index(4))
                if down > 2:
                    send(line, k, -1, away.index(-3))
            waiting[index] -= 1
            if waiting[index] == 0:
                start(buf.at[c, line], buf.at[c, line], d_s, d_r, partner)

        for near in (2, 1):
            for k in range(pieces):
                for s in (near, -near):
                    if s in away:
                        send(a, k, s, away.index(s))
        start(buf.at[c, a], buf.at[c, a], d_s, d_r, partner)
        events = list(extra)
        late = {1: 5.0, 2: 3.4, 3: 6.4, 4: 7.4}
        for s in away:
            for k in range(pieces):
                events.append((late[abs(s)] + 0.5 * k, functools.partial(step, s, k)))
        for order, (_, event) in enumerate(sorted(events, key=lambda pair: pair[0])):
            event()

    def drained(buf, a_s, a_r, d_s, d_r):
        sent(buf.at[c, pl.ds(0, n - 1)], a_s, a_r)
        sent(buf.at[c], d_s, d_r)

    spread(gall, ga_s, ga_r, gd_s, gd_r, ())
    sent(gall.at[c, a, pl.ds(0, (n - 1) * per)], gb_s, gb_r)
    arrived(gall.at[other], gd_s, gd_r)

    sources = (x, x, None, None, None, None, around(x + 2, nx), around(x + 2, nx))
    sides = (around(x - 1, nx), around(x + 1, nx))
    rows = left.shape[1]
    left_done = jnp.zeros((n * rows, 2 * value_width), jnp.float32)
    for g in range(GROUPS):
        columns = []
        for i in range(2):
            source = sides[i] if sources[g] is None else sources[g]
            at = pl.multiple_of((source * 4 + CHUNK[g][i]) * ch, ch)
            columns.append(left[:, :, pl.ds(at, ch)].reshape(n * rows, ch))
        grown = gall[:, :, g].reshape(2 * value_width, 2 * ch)
        left_done = left_done + dot(jnp.concatenate(columns, axis=1), grown, NT)

    high = left_done.astype(jnp.bfloat16)
    rest = left_done - high.astype(jnp.float32)
    middle = rest.astype(jnp.bfloat16)
    low = (rest - middle.astype(jnp.float32)).astype(jnp.bfloat16)
    done = []
    for h in range(2):
        columns = slice(h * value_width, (h + 1) * value_width)
        root = right[columns, :]
        done.append(dot(high[:, columns], root) + (dot(middle[:, columns], root) + dot(low[:, columns], root)))
    preconditioned = jnp.concatenate(done, axis=1)
    grown_line[...] = preconditioned.reshape(grown_line.shape)
    fresh = momentum_decay * momentum[...] + (1.0 - momentum_decay) * preconditioned.reshape(grown_line.shape)
    mall[c, a] = fresh.astype(jnp.bfloat16)

    def offered(value, slots, send, recv, where, at, size):
        slots[at] = value
        for d in range(1, size):
            start(slots.at[at], slots.at[at], send, recv, where(around(at + d, size)))

    stages = (
        (ssx, sx_s, sx_r, at_x, x, nx), (ssa, sa_s, sa_r, at_a, a, n), (ssd, sd_s, sd_r, lambda p: partner, c, 2),
    )
    squares = jnp.sum(jnp.sum(fresh * fresh, axis=0), keepdims=True)
    offered(jnp.broadcast_to(squares, ssx.shape[1:]), *stages[0])
    total = []

    def pass_on(index):
        slots, send, recv, _, _, size = stages[index]
        arrived(slots.at[pl.ds(0, size - 1)], send, recv)
        squares = jnp.sum(slots[...], axis=0)
        if index + 1 < len(stages):
            offered(squares, *stages[index + 1])
        else:
            total.append(squares)

    spread(mall, ma_s, ma_r, md_s, md_r,
           [(when, functools.partial(pass_on, index)) for index, when in enumerate((2.8, 6.6, 9.3))])
    factor = clip_level * lax.rsqrt(total[0] / entries + epsilon)
    factor_out[...] = jnp.broadcast_to(factor[0:1, 0:1], factor_out.shape)
    grown_out[...] = grown_line[b]
    weight_lines(4)
    arrived(wall.at[other], wd_s, wd_r)
    scale = factor[0:1, 0:1].reshape(1, 1, 1)

    def final(core, line):
        held = wall[core, line]
        step = scale * mall[core, line].astype(jnp.float32) + weight_decay * held
        return (held - step_rate * step).astype(jnp.bfloat16)

    arrived(mall.at[other], md_s, md_r)

    def laid(i, carry):
        copy_out[i, :, 0] = final(0, i)
        copy_out[:, i, 1] = final(1, i)
        return carry

    lax.fori_loop(0, n, laid, 0)
    drained(gall, ga_s, ga_r.at[0, 0], gd_s, gd_r)
    drained(mall, ma_s, ma_r.at[0, 0], md_s, md_r)
    drained(wall, wa_s, wa_r.at[0], wd_s, wd_r)
    for slots, send, recv, _, _, size in stages:
        sent(slots.at[pl.ds(0, size - 1)], send, recv)


def local(
    query_one, key_one, query_two, key_two, values, mix_ratio, head_gain,
    cotangent, left_roots, right_roots, weight, momentum,
):
    n = lax.axis_size("fs_0")
    nx = lax.axis_size("tp")
    tokens, own_cols = cotangent.shape
    rows = weight.shape[0]
    width = values.shape[1] // 2
    parts = width // n
    pair = own_cols // 2
    bf16, f32 = jnp.bfloat16, jnp.float32
    dma = pltpu.SemaphoreType.DMA
    vmem = pl.BlockSpec(memory_space=pltpu.VMEM)
    hbm = pl.BlockSpec(memory_space=pltpu.HBM)
    tile = (8, 128)
    shapes = pltpu.VMEM
    gain, mix = head_gain.reshape(1, -1), mix_ratio.reshape(1, -1)
    scratch = [
        shapes(array.shape, array.dtype)
        for array in (query_one, key_one, query_two, key_two, values, mix, gain, cotangent, right_roots)
    ]
    scratch += [
        dma((12,)),
        shapes((GROUPS - 2, tokens, pair), bf16),
        shapes((GROUPS, tokens, pair), bf16),
        shapes((width, tokens), bf16),
        shapes((width, tokens), bf16),
        shapes((width, tokens), bf16),
        shapes((GROUPS, n, parts, pair), bf16),
        shapes((GROUPS, n, parts, pair), bf16),
        shapes((GROUPS, parts, pair), bf16),
        shapes((n, GROUPS // n, parts, pair), bf16),
        shapes((2, n, GROUPS, parts, pair), bf16),
        shapes((2, n, n, rows, own_cols), f32),
        shapes((2, n, n, rows, own_cols), bf16),
        shapes((nx, *tile), f32),
        shapes((n, *tile), f32),
        shapes((2, *tile), f32),
        shapes((n, *left_roots.shape), bf16),
        shapes((n, rows, own_cols), f32),
        shapes((n, rows, own_cols), f32),
    ]
    pieces = min(4, n)
    for received in (
        (GROUPS - 2,), (GROUPS,), (), (GROUPS,), (), (), (n - 1, pieces), (), (n - 1, pieces), (),
        (), (n - 1,), (), (), (), (), (), (),
    ):
        scratch += [dma, dma(received) if received else dma]
    inputs = [
        pltpu.with_memory_space_constraint(array, pltpu.HBM)
        for array in (
            query_one, key_one, query_two, key_two, values, mix, gain,
            cotangent, left_roots, right_roots, weight, momentum,
        )
    ]
    grown, factor, copied = pl.pallas_call(
        functools.partial(kernel, float(weight.size * n * n * 2 * nx)),
        out_shape=(
            jax.ShapeDtypeStruct(weight.shape, f32),
            jax.ShapeDtypeStruct(weight.shape, f32),
            jax.ShapeDtypeStruct((n, n, 2, rows, own_cols), bf16),
        ),
        in_specs=[hbm] * 12,
        out_specs=[vmem] * 3,
        scratch_shapes=scratch,
        compiler_params=pltpu.CompilerParams(
            collective_id=0, has_side_effects=True, vmem_limit_bytes=40 * 1024 * 1024
        ),
    )(*inputs)
    momentum_new = momentum_decay * momentum + (1.0 - momentum_decay) * grown
    step = factor * momentum_new + weight_decay * weight
    weight_new = weight - step_rate * step
    return step, weight_new, momentum_new, copied.reshape(-1, own_cols)


def split_mesh(mesh):
    lines = int((mesh.shape["fs"] // 2) ** 0.5)
    return Mesh(mesh.devices.reshape(lines, lines, 2, mesh.shape["tp"]), (*FS, "tp"))


def solution(mesh):
    return jax.shard_map(
        local,
        mesh=split_mesh(mesh),
        in_specs=(
            P(FS, "tp"), P(FS, "tp"), P(FS, "tp"), P(FS, "tp"), P(FS, "tp"), P("tp"), P(),
            P(FS, "tp"), P(FS, None), P("tp", None), P(FS, "tp"), P(FS, "tp"),
        ),
        out_specs=(P(FS, "tp"), P(FS, "tp"), P(FS, "tp"), P(None, "tp")),
        check_vma=False,
    )
```

```python
import functools

import jax
import jax.numpy as jnp
from jax import lax
from jax.experimental import pallas as pl
from jax.experimental.pallas import tpu as pltpu
from jax.sharding import Mesh
from jax.sharding import PartitionSpec as P

FS = ("fs_0", "fs_1", "fs_2")
MESH_ID = pl.DeviceIdType.MESH

epsilon = 1e-06
momentum_decay = 0.8
clip_level = 0.5
weight_decay = 0.2
step_rate = 0.1

GROUPS = 8
LAST = 3
CHUNK = ((0, 1), (2, 3), (0, 2), (1, 3), (2, 0), (3, 1), (0, 2), (1, 3))
NT = (((1,), (1,)), ((), ()))


def dot(left, right, dims=(((1,), (0,)), ((), ()))):
    return lax.dot_general(left, right, dims, preferred_element_type=jnp.float32)


def kernel(
    entries,
    q1_in, k1_in, q2_in, k2_in, val_in, mix_in, gain_in, cot_in, left_in, right_in, weight_in, momentum_in,
    grown_out, factor_out, copy_out,
    q1, k1, q2, k2, val, mix, gain, cot, right, load,
    cm, cp, at_own, at_send, at_part, gsend, rs1, s1b, rs2, rsb, gall, wall, mall, ssx, ssa, ssd,
    left, momentum, grown_line,
    x_s, x_r, c_s, c_r, a_s, a_r, r1_s, r1_r, r2_s, r2_r, rb_s, rb_r,
    gb_s, gb_r, ga_s, ga_r, gd_s, gd_r, ma_s, ma_r, md_s, md_r,
    wb_s, wb_r, wa_s, wa_r, wd_s, wd_r, lb_s, lb_r, lx_s, lx_r, pb_s, pb_r,
    sx_s, sx_r, sa_s, sa_r, sd_s, sd_r,
):
    z, y, c, x = (lax.axis_index(name) for name in (*FS, "tp"))
    n = rs2.shape[0]
    nx = ssx.shape[0]
    other = 1 - c
    a = z * other + y * c
    b = y * other + z * c

    def at_a(p):
        return (p * other + z * c, y * other + p * c, c, x)

    def at_b(p):
        return (z * other + p * c, p * other + y * c, c, x)

    def at_x(p):
        return (z, y, c, p)

    partner = (z, y, other, x)

    def remote(src, dst, send, recv, where):
        return pltpu.make_async_remote_copy(
            src_ref=src, dst_ref=dst, send_sem=send, recv_sem=recv,
            device_id=where, device_id_type=MESH_ID,
        )

    def start(*parts):
        remote(*parts).start()

    def arrived(dst, send, recv):
        remote(dst, dst, send, recv, partner).wait_recv()

    def sent(src, send, recv):
        remote(src, src, send, recv, partner).wait_send()

    def around(p, size):
        return lax.rem(p + size, size)

    loads = {}
    for i, (name, src, dst) in enumerate((
        ("cot", cot_in, cot), ("q1", q1_in, q1), ("k1", k1_in, k1), ("q2", q2_in, q2), ("k2", k2_in, k2),
        ("val", val_in, val), ("gain", gain_in, gain), ("mix", mix_in, mix), ("weight", weight_in, wall.at[c, a, b]),
        ("left", left_in.at[:, pl.ds(pl.multiple_of(x * cot.shape[1], cot.shape[1]), cot.shape[1])], left.at[0, b]), ("right", right_in, right), ("momentum", momentum_in, momentum.at[b]),
    )):
        loads[name] = pltpu.make_async_copy(src, dst, load.at[i])
        loads[name].start()

    barrier = pltpu.get_barrier_semaphore()
    peers = [partner]
    for d in range(1, n):
        peers += [at_a(around(a + d, n)), at_b(around(b + d, n))]
    for d in range(1, nx):
        peers.append(at_x(around(x + d, nx)))
    for peer in peers:
        pl.semaphore_signal(barrier, inc=1, device_id=peer, device_id_type=MESH_ID)
    pl.semaphore_wait(barrier, len(peers))

    tokens = cot.shape[0]
    ch = cot.shape[1] // 4
    ahead = at_x(around(x + 1, nx))
    behind = at_x(around(x - 1, nx))

    def half(i):
        return pl.ds(i * ch, ch)

    loads["cot"].wait()
    for g in range(2, 6):
        for i, where in ((0, ahead), (1, behind)):
            start(cot.at[:, half(CHUNK[g][i])], cm.at[g - 2, :, half(i)], x_s, x_r.at[g - 2], where)
    for g in range(2):
        start(cot.at[:, pl.ds(2 * g * ch, 2 * ch)], cp.at[g], c_s, c_r.at[g], partner)
    up = n // 2
    down = n - 1 - up
    away = list(range(1, up + 1)) + [-d for d in range(1, down + 1)]
    for name, held, send, recv in (
        ("weight", wall.at[c, a, b], wb_s, wb_r), ("momentum", momentum.at[b], pb_s, pb_r),
    ):
        loads[name].wait()
        for d in range(1, n):
            start(held, held, send, recv, at_b(around(b + d, n)))
    loads["left"].wait()
    for d in range(1, n):
        start(left.at[0, b], left.at[0, b], lb_s, lb_r, at_b(around(b + d, n)))

    for name in ("q1", "k1", "q2", "k2", "val", "gain", "mix"):
        loads[name].wait()
    key_width = q1.shape[1] // 2
    value_width = val.shape[1] // 2
    block = tokens // 5

    def attend(h, out):
        chosen = lax.broadcasted_iota(jnp.int32, (1, 2), 1) == h
        ratio = jnp.sum(jnp.where(chosen, mix[...], 0.0), axis=1, keepdims=True)
        keyed = pl.ds(pl.multiple_of(h * key_width, key_width), key_width)
        valued = pl.ds(pl.multiple_of(h * value_width, value_width), value_width)
        for at in range(5):
            low, high = at * block, (at + 1) * block
            rows = lax.broadcasted_iota(jnp.int32, (block, high), 0) + low
            seen = lax.broadcasted_iota(jnp.int32, (block, high), 1) <= rows

            def probs(query, keys):
                scores = dot(query[low:high, keyed], keys[0:high, keyed], NT) * key_width ** (-0.5)
                scores = jnp.where(seen, scores, -jnp.inf)
                grown = jnp.exp(scores - jnp.max(scores, axis=1, keepdims=True))
                return grown, 1.0 / jnp.sum(grown, axis=1, keepdims=True)

            one, one_scale = probs(q1, k1)
            two, two_scale = probs(q2, k2)
            mixed = (one * one_scale - ratio * (two * two_scale)).astype(jnp.bfloat16)
            head = dot(mixed, val[0:high, valued])
            square = jnp.mean(head * head, axis=1, keepdims=True)
            normed = head * lax.rsqrt(square + epsilon) * gain[...]
            out[:, low:high] = normed.T.astype(jnp.bfloat16)

    def take(g):
        arrived(cm.at[g - 2], x_s, x_r.at[g - 2])
        if g < 4:
            for i, where in ((0, ahead), (1, behind)):
                start(cm.at[g - 2, :, half(i)], cm.at[g + 2, :, half(i)], x_s, x_r.at[g + 2], where)
        start(cm.at[g - 2], cp.at[g], c_s, c_r.at[g], partner)

    steps = [(h, 1, h == up) for h in range(1, up + 1)] + [(h, -1, h == n - 1 - up) for h in range(1, n - up)]

    def line_of(index, home):
        h, way, _ = steps[index]
        return around(home - way * h, n)

    def weight_lines(h):
        for index, (hop, way, last) in enumerate(steps):
            if hop != h:
                continue
            line = wall.at[c, line_of(index, a)]
            arrived(line, wa_s, wa_r.at[index])
            if not last:
                start(line, line, wa_s, wa_r.at[index + 1], at_a(around(a + way, n)))
            start(line, line, wd_s, wd_r, partner)

    attend(other, at_send)
    start(at_send, at_part, a_s, a_r, partner)
    attend(c, at_own)
    arrived(at_part, a_s, a_r)

    parts = gsend.shape[2]
    others = pl.ds(1, n - 1)

    def summed(g):
        arrived(rs1.at[g, others], r1_s, r1_r.at[g])
        total = rs1[g, 0].astype(jnp.float32)
        for d in range(1, n):
            total = total + rs1[g, d].astype(jnp.float32)
        s1b[g] = total.astype(jnp.bfloat16)

    per = GROUPS // n

    early = GROUPS - LAST

    def owned(p):
        return len([g for g in range(early) if g // per == p])

    def finish(g):
        summed(g)
        if g >= early:
            rsb[g - early, b] = s1b[g]
            for d in range(1, n):
                start(s1b.at[g], rsb.at[g - early, b], rb_s, rb_r.at[g - early], at_b(around(b + d, n)))
            return
        owner = g // per

        @pl.when(b != owner)
        def _():
            start(s1b.at[g], rs2.at[around(b - owner, n), g % per], r2_s, r2_r.at[g % per], at_b(owner))

    def own(g):
        @pl.when(b == g // per)
        def _():
            arrived(rs2.at[others, g % per], r2_s, r2_r.at[g % per])
            total = s1b[g].astype(jnp.float32)
            for d in range(1, n):
                total = total + rs2[d, g % per].astype(jnp.float32)
            gall[c, a, g] = total.astype(jnp.bfloat16)
            for d in range(1, n):
                start(gall.at[c, a, g], gall.at[c, a, g], gb_s, gb_r.at[g], at_b(around(b + d, n)))

    def whole(g):
        if g >= early:
            arrived(rsb.at[g - early, others], rb_s, rb_r.at[g - early])
            total = rsb[g - early, 0].astype(jnp.float32)
            for p in range(1, n):
                total = total + rsb[g - early, p].astype(jnp.float32)
            gall[c, a, g] = total.astype(jnp.bfloat16)
            return

        @pl.when(b != g // per)
        def _():
            arrived(gall.at[c, a, g], gb_s, gb_r.at[g])

    for g in range(GROUPS):
        if g >= 2:
            take(g)
        if g == 2:
            arrived(wall.at[c, a, pl.ds(0, n - 1)], wb_s, wb_r)
            line = wall.at[c, a]
            for index, (h, way, _) in enumerate(steps):
                if h == 1:
                    start(line, line, wa_s, wa_r.at[index], at_a(around(a + way, n)))
            start(line, line, wd_s, wd_r, partner)
        mine = cot[:, 2 * g * ch : 2 * (g + 1) * ch] if g < 2 else cm[g - 2]
        grad = dot(at_own[...], mine)
        arrived(cp.at[g], c_s, c_r.at[g])
        grad = grad + dot(at_part[...], cp[g])
        gsend[g] = grad.reshape(n, parts, 2 * ch).astype(jnp.bfloat16)
        rs1[g, 0] = gsend[g, a]
        for d in range(1, n):
            p = around(a + d, n)
            start(gsend.at[g, p], rs1.at[g, d], r1_s, r1_r.at[g], at_a(p))
        if g == 5:
            weight_lines(1)
        if g >= 5:
            finish(g - 5)
    arrived(left.at[0, pl.ds(0, n - 1)], lb_s, lb_r)
    for d in range(1, nx):
        start(left.at[0], left.at[d], lx_s, lx_r, at_x(around(x + d, nx)))
    sent(cm, x_s, x_r.at[0])
    sent(cp, c_s, c_r.at[0])
    sent(at_send, a_s, a_r)
    sent(wall.at[c, a, pl.ds(0, n - 1)], wb_s, wb_r)
    sent(momentum.at[pl.ds(0, n - 1)], pb_s, pb_r)
    arrived(momentum.at[pl.ds(0, n - 1)], pb_s, pb_r)
    sent(left.at[0, pl.ds(0, n - 1)], lb_s, lb_r)
    loads["right"].wait()
    finish(3)
    finish(4)
    own(0)
    own(1)
    own(2)
    finish(5)
    own(3)
    finish(6)
    own(4)
    finish(7)

    weight_lines(2)

    def spread(buf, a_s, a_r, d_s, d_r, entries, extra):
        pieces = a_r.shape[1]
        count = buf.shape[2] // pieces
        waiting = [pieces] * (len(away) + 1)

        def done(index, line):
            waiting[index] -= 1
            if waiting[index] == 0:
                start(buf.at[c, line], buf.at[c, line], d_s, d_r, partner)

        def send(line, k, to, index):
            part = buf.at[c, line, pl.ds(k * count, count)]
            start(part, part, a_s, a_r.at[index, k], at_a(around(a + to, n)))

        def enter(k, ready):
            ready()
            for s in (2, -2, 1, -1):
                if s in away:
                    send(a, k, s, away.index(s))
            done(len(away), a)

        def step(s, k):
            index = away.index(s)
            line = around(a - s, n)
            arrived(buf.at[c, line, pl.ds(k * count, count)], a_s, a_r.at[index, k])
            if s == 2:
                if up > 3 and k % 2 == 0:
                    send(line, k, 2, away.index(4))
                if up > 2:
                    send(line, k, 1, away.index(3))
            if s == -2:
                if up > 3 and k % 2 == 1:
                    send(line, k, -2, away.index(4))
                if down > 2:
                    send(line, k, -1, away.index(-3))
            done(index, line)

        events = list(extra)
        late = {1: 5.0, 2: 3.6, 3: 6.4, 4: 7.4}
        for k in range(pieces):
            when, ready = entries[k]
            events.append((when, functools.partial(enter, k, ready)))
            for s in away:
                events.append((when + late[abs(s)], functools.partial(step, s, k)))
        for order, (_, event) in enumerate(sorted(events, key=lambda pair: pair[0])):
            event()

    pieces = ga_r.shape[1]
    count = GROUPS // pieces

    def whole_piece(k):
        for g in range(k * count, (k + 1) * count):
            whole(g)

    def drained(buf, a_s, a_r, d_s, d_r):
        sent(buf.at[c, pl.ds(0, n - 1)], a_s, a_r)
        sent(buf.at[c], d_s, d_r)

    spread(
        gall, ga_s, ga_r, gd_s, gd_r, [(0.1 * k, functools.partial(whole_piece, k)) for k in range(pieces)],
        [(4.0, lambda: weight_lines(3))],
    )
    sent(rs1.at[:, others], r1_s, r1_r.at[0])
    sent(rsb.at[:, others], rb_s, rb_r.at[0])
    for p in range(n):
        @pl.when(b == p)
        def _():
            sent(s1b.at[pl.ds(0, early - owned(p))], r2_s, r2_r.at[0])
            if owned(p):
                sent(gall.at[c, a, pl.ds(0, (n - 1) * owned(p))], gb_s, gb_r.at[0])

    arrived(gall.at[other], gd_s, gd_r)

    slots = ((0, 0), (0, 0), *(((1, nx - 1),) * 4), (2, 2), (2, 2))
    arrived(left.at[pl.ds(1, nx - 1)], lx_s, lx_r)
    rows = left.shape[2]
    left_done = jnp.zeros((n * rows, 2 * value_width), jnp.float32)
    for g in range(GROUPS):
        columns = [
            left[slots[g][i], :, :, CHUNK[g][i] * ch : (CHUNK[g][i] + 1) * ch].reshape(n * rows, ch) for i in range(2)
        ]
        grown = gall[:, :, g].reshape(2 * value_width, 2 * ch)
        left_done = left_done + dot(jnp.concatenate(columns, axis=1), grown, NT)

    high = left_done.astype(jnp.bfloat16)
    rest = left_done - high.astype(jnp.float32)
    middle = rest.astype(jnp.bfloat16)
    low = (rest - middle.astype(jnp.float32)).astype(jnp.bfloat16)
    done = []
    for h in range(2):
        columns = slice(h * value_width, (h + 1) * value_width)
        root = right[columns, :]
        done.append(dot(high[:, columns], root) + (dot(middle[:, columns], root) + dot(low[:, columns], root)))
    preconditioned = jnp.concatenate(done, axis=1)
    grown_line[...] = preconditioned.reshape(grown_line.shape)
    fresh = momentum_decay * momentum[...] + (1.0 - momentum_decay) * preconditioned.reshape(grown_line.shape)
    mall[c, a] = fresh.astype(jnp.bfloat16)

    def offered(value, slots, send, recv, where, at, size):
        slots[at] = value
        for d in range(1, size):
            start(slots.at[at], slots.at[at], send, recv, where(around(at + d, size)))

    stages = (
        (ssx, sx_s, sx_r, at_x, x, nx), (ssa, sa_s, sa_r, at_a, a, n), (ssd, sd_s, sd_r, lambda p: partner, c, 2),
    )
    squares = jnp.sum(jnp.sum(fresh * fresh, axis=0), keepdims=True)
    offered(jnp.broadcast_to(squares, ssx.shape[1:]), *stages[0])
    total = []

    def pass_on(index):
        slots, send, recv, _, _, size = stages[index]
        arrived(slots.at[pl.ds(0, size - 1)], send, recv)
        squares = jnp.sum(slots[...], axis=0)
        if index + 1 < len(stages):
            offered(squares, *stages[index + 1])
        else:
            total.append(squares)

    spread(
        mall, ma_s, ma_r, md_s, md_r, [(0.35 * k, lambda: None) for k in range(ma_r.shape[1])],
        [(4.7, lambda: weight_lines(4)), *((when, functools.partial(pass_on, index)) for index, when in enumerate((2.8, 6.6, 9.3)))],
    )
    factor = clip_level * lax.rsqrt(total[0] / entries + epsilon)
    factor_out[...] = jnp.broadcast_to(factor[0:1, 0:1], factor_out.shape)
    grown_out[...] = grown_line[b]
    arrived(wall.at[other], wd_s, wd_r)
    scale = factor[0:1, 0:1].reshape(1, 1, 1)

    def final(core, line):
        held = wall[core, line]
        step = scale * mall[core, line].astype(jnp.float32) + weight_decay * held
        return (held - step_rate * step).astype(jnp.bfloat16)

    arrived(mall.at[other], md_s, md_r)

    def laid(i, carry):
        copy_out[i, :, 0] = final(0, i)
        copy_out[:, i, 1] = final(1, i)
        return carry

    lax.fori_loop(0, n, laid, 0)
    drained(gall, ga_s, ga_r.at[0, 0], gd_s, gd_r)
    drained(mall, ma_s, ma_r.at[0, 0], md_s, md_r)
    sent(left.at[pl.ds(1, nx - 1)], lx_s, lx_r)
    drained(wall, wa_s, wa_r.at[0], wd_s, wd_r)
    for slots, send, recv, _, _, size in stages:
        sent(slots.at[pl.ds(0, size - 1)], send, recv)


def local(
    query_one, key_one, query_two, key_two, values, mix_ratio, head_gain,
    cotangent, left_roots, right_roots, weight, momentum,
):
    n = lax.axis_size("fs_0")
    nx = lax.axis_size("tp")
    tokens, own_cols = cotangent.shape
    rows = weight.shape[0]
    width = values.shape[1] // 2
    parts = width // n
    pair = own_cols // 2
    bf16, f32 = jnp.bfloat16, jnp.float32
    dma = pltpu.SemaphoreType.DMA
    vmem = pl.BlockSpec(memory_space=pltpu.VMEM)
    hbm = pl.BlockSpec(memory_space=pltpu.HBM)
    tile = (8, 128)
    shapes = pltpu.VMEM
    gain, mix = head_gain.reshape(1, -1), mix_ratio.reshape(1, -1)
    scratch = [
        shapes(array.shape, array.dtype)
        for array in (query_one, key_one, query_two, key_two, values, mix, gain, cotangent, right_roots)
    ]
    scratch += [
        dma((12,)),
        shapes((GROUPS - 2, tokens, pair), bf16),
        shapes((GROUPS, tokens, pair), bf16),
        shapes((width, tokens), bf16),
        shapes((width, tokens), bf16),
        shapes((width, tokens), bf16),
        shapes((GROUPS, n, parts, pair), bf16),
        shapes((GROUPS, n, parts, pair), bf16),
        shapes((GROUPS, parts, pair), bf16),
        shapes((n, GROUPS // n, parts, pair), bf16),
        shapes((LAST, n, parts, pair), bf16),
        shapes((2, n, GROUPS, parts, pair), bf16),
        shapes((2, n, n, rows, own_cols), f32),
        shapes((2, n, n, rows, own_cols), bf16),
        shapes((nx, *tile), f32),
        shapes((n, *tile), f32),
        shapes((2, *tile), f32),
        shapes((nx, n, rows, own_cols), bf16),
        shapes((n, rows, own_cols), f32),
        shapes((n, rows, own_cols), f32),
    ]
    pieces = min(4, n)
    for received in (
        (GROUPS - 2,), (GROUPS,), (), (GROUPS,), (GROUPS // n,), (LAST,), (GROUPS,), (n - 1, pieces), (), (n - 1, pieces), (),
        (), (n - 1,), (), (), (), (), (), (), (),
    ):
        scratch += [dma, dma(received) if received else dma]
    inputs = [
        pltpu.with_memory_space_constraint(array, pltpu.HBM)
        for array in (
            query_one, key_one, query_two, key_two, values, mix, gain,
            cotangent, left_roots, right_roots, weight, momentum,
        )
    ]
    grown, factor, copied = pl.pallas_call(
        functools.partial(kernel, float(weight.size * n * n * 2 * nx)),
        out_shape=(
            jax.ShapeDtypeStruct(weight.shape, f32),
            jax.ShapeDtypeStruct(weight.shape, f32),
            jax.ShapeDtypeStruct((n, n, 2, rows, own_cols), bf16),
        ),
        in_specs=[hbm] * 12,
        out_specs=[vmem] * 3,
        scratch_shapes=scratch,
        compiler_params=pltpu.CompilerParams(
            collective_id=0, has_side_effects=True, vmem_limit_bytes=40 * 1024 * 1024
        ),
    )(*inputs)
    momentum_new = momentum_decay * momentum + (1.0 - momentum_decay) * grown
    step = factor * momentum_new + weight_decay * weight
    weight_new = weight - step_rate * step
    return step, weight_new, momentum_new, copied.reshape(-1, own_cols)


def split_mesh(mesh):
    lines = int((mesh.shape["fs"] // 2) ** 0.5)
    return Mesh(mesh.devices.reshape(lines, lines, 2, mesh.shape["tp"]), (*FS, "tp"))


def solution(mesh):
    return jax.shard_map(
        local,
        mesh=split_mesh(mesh),
        in_specs=(
            P(FS, "tp"), P(FS, "tp"), P(FS, "tp"), P(FS, "tp"), P(FS, "tp"), P("tp"), P(),
            P(FS, "tp"), P(FS, None), P("tp", None), P(FS, "tp"), P(FS, "tp"),
        ),
        out_specs=(P(FS, "tp"), P(FS, "tp"), P(FS, "tp"), P(None, "tp")),
        check_vma=False,
    )
```

```python
import functools

import jax
import jax.numpy as jnp
from jax import lax
from jax.experimental import pallas as pl
from jax.experimental.pallas import tpu as pltpu
from jax.sharding import Mesh
from jax.sharding import PartitionSpec as P

FS = ("fs_0", "fs_1", "fs_2")
MESH_ID = pl.DeviceIdType.MESH

epsilon = 1e-06
momentum_decay = 0.8
clip_level = 0.5
weight_decay = 0.2
step_rate = 0.1

GROUPS = 8
LAST = 4
CHUNK = ((0, 1), (2, 3), (0, 2), (1, 3), (2, 0), (3, 1), (0, 2), (1, 3))
NT = (((1,), (1,)), ((), ()))


def dot(left, right, dims=(((1,), (0,)), ((), ()))):
    return lax.dot_general(left, right, dims, preferred_element_type=jnp.float32)


def kernel(
    entries,
    q1_in, k1_in, q2_in, k2_in, val_in, mix_in, gain_in, cot_in, left_in, right_in, weight_in, momentum_in,
    grown_out, factor_out, copy_out,
    q1, k1, q2, k2, val, mix, gain, cot, right, load,
    cm, cp, at_own, at_send, at_part, gsend, rs1, s1b, rs2, rsb, gall, wall, mall, ssx, ssa, ssd,
    left, momentum, grown_line,
    x_s, x_r, c_s, c_r, a_s, a_r, r1_s, r1_r, r2_s, r2_r, rb_s, rb_r,
    gb_s, gb_r, ga_s, ga_r, gd_s, gd_r, ma_s, ma_r, md_s, md_r,
    wb_s, wb_r, wa_s, wa_r, wd_s, wd_r, lb_s, lb_r, lx_s, lx_r, pb_s, pb_r,
    sx_s, sx_r, sa_s, sa_r, sd_s, sd_r,
):
    z, y, c, x = (lax.axis_index(name) for name in (*FS, "tp"))
    n = rs2.shape[0]
    nx = ssx.shape[0]
    other = 1 - c
    a = z * other + y * c
    b = y * other + z * c

    def at_a(p):
        return (p * other + z * c, y * other + p * c, c, x)

    def at_b(p):
        return (z * other + p * c, p * other + y * c, c, x)

    def at_x(p):
        return (z, y, c, p)

    partner = (z, y, other, x)

    def remote(src, dst, send, recv, where):
        return pltpu.make_async_remote_copy(
            src_ref=src, dst_ref=dst, send_sem=send, recv_sem=recv,
            device_id=where, device_id_type=MESH_ID,
        )

    def start(*parts):
        remote(*parts).start()

    def arrived(dst, send, recv):
        remote(dst, dst, send, recv, partner).wait_recv()

    def sent(src, send, recv):
        remote(src, src, send, recv, partner).wait_send()

    def around(p, size):
        return lax.rem(p + size, size)

    loads = {}
    for i, (name, src, dst) in enumerate((
        ("cot", cot_in, cot), ("q1", q1_in, q1), ("k1", k1_in, k1), ("q2", q2_in, q2), ("k2", k2_in, k2),
        ("val", val_in, val), ("gain", gain_in, gain), ("mix", mix_in, mix), ("weight", weight_in, wall.at[c, a, b]),
        ("left", left_in.at[:, pl.ds(pl.multiple_of(x * cot.shape[1], cot.shape[1]), cot.shape[1])], left.at[0, b]), ("right", right_in, right), ("momentum", momentum_in, momentum.at[b]),
    )):
        loads[name] = pltpu.make_async_copy(src, dst, load.at[i])
        loads[name].start()

    barrier = pltpu.get_barrier_semaphore()
    peers = [partner]
    for d in range(1, n):
        peers += [at_a(around(a + d, n)), at_b(around(b + d, n))]
    for d in range(1, nx):
        peers.append(at_x(around(x + d, nx)))
    for peer in peers:
        pl.semaphore_signal(barrier, inc=1, device_id=peer, device_id_type=MESH_ID)
    pl.semaphore_wait(barrier, len(peers))

    tokens = cot.shape[0]
    ch = cot.shape[1] // 4
    ahead = at_x(around(x + 1, nx))
    behind = at_x(around(x - 1, nx))

    def half(i):
        return pl.ds(i * ch, ch)

    loads["cot"].wait()
    for g in range(2, 6):
        for i, where in ((0, ahead), (1, behind)):
            start(cot.at[:, half(CHUNK[g][i])], cm.at[g - 2, :, half(i)], x_s, x_r.at[g - 2], where)
    for g in range(2):
        start(cot.at[:, pl.ds(2 * g * ch, 2 * ch)], cp.at[g], c_s, c_r.at[g], partner)
    up = n // 2
    down = n - 1 - up
    away = list(range(1, up + 1)) + [-d for d in range(1, down + 1)]
    for name, held, send, recv in (
        ("weight", wall.at[c, a, b], wb_s, wb_r), ("momentum", momentum.at[b], pb_s, pb_r),
    ):
        loads[name].wait()
        for d in range(1, n):
            start(held, held, send, recv, at_b(around(b + d, n)))
    loads["left"].wait()
    for d in range(1, n):
        start(left.at[0, b], left.at[0, b], lb_s, lb_r, at_b(around(b + d, n)))

    for name in ("q1", "k1", "q2", "k2", "val", "gain", "mix"):
        loads[name].wait()
    key_width = q1.shape[1] // 2
    value_width = val.shape[1] // 2
    block = tokens // 5

    def attend(h, out):
        chosen = lax.broadcasted_iota(jnp.int32, (1, 2), 1) == h
        ratio = jnp.sum(jnp.where(chosen, mix[...], 0.0), axis=1, keepdims=True)
        keyed = pl.ds(pl.multiple_of(h * key_width, key_width), key_width)
        valued = pl.ds(pl.multiple_of(h * value_width, value_width), value_width)
        for at in range(5):
            low, high = at * block, (at + 1) * block
            rows = lax.broadcasted_iota(jnp.int32, (block, high), 0) + low
            seen = lax.broadcasted_iota(jnp.int32, (block, high), 1) <= rows

            def probs(query, keys):
                scores = dot(query[low:high, keyed], keys[0:high, keyed], NT) * key_width ** (-0.5)
                scores = jnp.where(seen, scores, -jnp.inf)
                grown = jnp.exp(scores - jnp.max(scores, axis=1, keepdims=True))
                return grown, 1.0 / jnp.sum(grown, axis=1, keepdims=True)

            one, one_scale = probs(q1, k1)
            two, two_scale = probs(q2, k2)
            mixed = (one * one_scale - ratio * (two * two_scale)).astype(jnp.bfloat16)
            head = dot(mixed, val[0:high, valued])
            square = jnp.mean(head * head, axis=1, keepdims=True)
            normed = head * lax.rsqrt(square + epsilon) * gain[...]
            out[:, low:high] = normed.T.astype(jnp.bfloat16)

    def take(g):
        arrived(cm.at[g - 2], x_s, x_r.at[g - 2])
        if g < 4:
            for i, where in ((0, ahead), (1, behind)):
                start(cm.at[g - 2, :, half(i)], cm.at[g + 2, :, half(i)], x_s, x_r.at[g + 2], where)
        start(cm.at[g - 2], cp.at[g], c_s, c_r.at[g], partner)

    steps = [(h, 1, h == up) for h in range(1, up + 1)] + [(h, -1, h == n - 1 - up) for h in range(1, n - up)]

    def line_of(index, home):
        h, way, _ = steps[index]
        return around(home - way * h, n)

    def weight_lines(h):
        for index, (hop, way, last) in enumerate(steps):
            if hop != h:
                continue
            line = wall.at[c, line_of(index, a)]
            arrived(line, wa_s, wa_r.at[index])
            if not last:
                start(line, line, wa_s, wa_r.at[index + 1], at_a(around(a + way, n)))
            start(line, line, wd_s, wd_r, partner)

    attend(other, at_send)
    start(at_send, at_part, a_s, a_r, partner)
    attend(c, at_own)
    arrived(at_part, a_s, a_r)

    parts = gsend.shape[2]
    others = pl.ds(1, n - 1)

    def summed(g):
        arrived(rs1.at[g, others], r1_s, r1_r.at[g])
        total = rs1[g, 0].astype(jnp.float32)
        for d in range(1, n):
            total = total + rs1[g, d].astype(jnp.float32)
        s1b[g] = total.astype(jnp.bfloat16)

    per = GROUPS // n

    early = GROUPS - LAST

    def owned(p):
        return len([g for g in range(early) if g // per == p])

    def finish(g):
        summed(g)
        if g >= early:
            rsb[g - early, b] = s1b[g]
            for d in range(1, n):
                start(s1b.at[g], rsb.at[g - early, b], rb_s, rb_r.at[g - early], at_b(around(b + d, n)))
            return
        owner = g // per

        @pl.when(b != owner)
        def _():
            start(s1b.at[g], rs2.at[around(b - owner, n), g % per], r2_s, r2_r.at[g % per], at_b(owner))

    def own(g):
        @pl.when(b == g // per)
        def _():
            arrived(rs2.at[others, g % per], r2_s, r2_r.at[g % per])
            total = s1b[g].astype(jnp.float32)
            for d in range(1, n):
                total = total + rs2[d, g % per].astype(jnp.float32)
            gall[c, a, g] = total.astype(jnp.bfloat16)
            for d in range(1, n):
                start(gall.at[c, a, g], gall.at[c, a, g], gb_s, gb_r.at[g], at_b(around(b + d, n)))

    def whole(g):
        if g >= early:
            arrived(rsb.at[g - early, others], rb_s, rb_r.at[g - early])
            total = rsb[g - early, 0].astype(jnp.float32)
            for p in range(1, n):
                total = total + rsb[g - early, p].astype(jnp.float32)
            gall[c, a, g] = total.astype(jnp.bfloat16)
            return

        @pl.when(b != g // per)
        def _():
            arrived(gall.at[c, a, g], gb_s, gb_r.at[g])

    for g in range(GROUPS):
        if g >= 2:
            take(g)
        if g == 2:
            arrived(wall.at[c, a, pl.ds(0, n - 1)], wb_s, wb_r)
            line = wall.at[c, a]
            for index, (h, way, _) in enumerate(steps):
                if h == 1:
                    start(line, line, wa_s, wa_r.at[index], at_a(around(a + way, n)))
            start(line, line, wd_s, wd_r, partner)
        mine = cot[:, 2 * g * ch : 2 * (g + 1) * ch] if g < 2 else cm[g - 2]
        grad = dot(at_own[...], mine)
        arrived(cp.at[g], c_s, c_r.at[g])
        grad = grad + dot(at_part[...], cp[g])
        gsend[g] = grad.reshape(n, parts, 2 * ch).astype(jnp.bfloat16)
        rs1[g, 0] = gsend[g, a]
        for d in range(1, n):
            p = around(a + d, n)
            start(gsend.at[g, p], rs1.at[g, d], r1_s, r1_r.at[g], at_a(p))
        if g == 5:
            weight_lines(1)
        for ended in {4: (0, 1), 5: (2,), 6: (3,), 7: (4,)}.get(g, ()):
            finish(ended)
        for ended in {6: (0, 1), 7: (2,)}.get(g, ()):
            own(ended)
    arrived(left.at[0, pl.ds(0, n - 1)], lb_s, lb_r)
    for d in range(1, nx):
        start(left.at[0], left.at[d], lx_s, lx_r, at_x(around(x + d, nx)))
    sent(cm, x_s, x_r.at[0])
    sent(cp, c_s, c_r.at[0])
    sent(at_send, a_s, a_r)
    sent(wall.at[c, a, pl.ds(0, n - 1)], wb_s, wb_r)
    sent(momentum.at[pl.ds(0, n - 1)], pb_s, pb_r)
    arrived(momentum.at[pl.ds(0, n - 1)], pb_s, pb_r)
    sent(left.at[0, pl.ds(0, n - 1)], lb_s, lb_r)
    loads["right"].wait()
    finish(5)
    own(3)
    finish(6)
    def spread(buf, a_s, a_r, d_s, d_r, entries, extra):
        pieces = a_r.shape[1]
        count = buf.shape[2] // pieces
        waiting = [pieces] * (len(away) + 1)

        def done(index, line):
            waiting[index] -= 1
            if waiting[index] == 0:
                start(buf.at[c, line], buf.at[c, line], d_s, d_r, partner)

        def send(line, k, to, index):
            part = buf.at[c, line, pl.ds(k * count, count)]
            start(part, part, a_s, a_r.at[index, k], at_a(around(a + to, n)))

        def enter(k, ready):
            ready()
            for s in (2, -2, 1, -1):
                if s in away:
                    send(a, k, s, away.index(s))
            done(len(away), a)

        def step(s, k):
            index = away.index(s)
            line = around(a - s, n)
            arrived(buf.at[c, line, pl.ds(k * count, count)], a_s, a_r.at[index, k])
            if s == 2:
                if up > 3 and k % 2 == 0:
                    send(line, k, 2, away.index(4))
                if up > 2:
                    send(line, k, 1, away.index(3))
            if s == -2:
                if up > 3 and k % 2 == 1:
                    send(line, k, -2, away.index(4))
                if down > 2:
                    send(line, k, -1, away.index(-3))
            done(index, line)

        events = list(extra)
        late = {1: 5.0, 2: 3.6, 3: 6.4, 4: 7.4}
        for k in range(pieces):
            when, ready = entries[k]
            events.append((when, functools.partial(enter, k, ready)))
            for s in away:
                events.append((when + late[abs(s)], functools.partial(step, s, k)))
        for order, (_, event) in enumerate(sorted(events, key=lambda pair: pair[0])):
            event()

    pieces = ga_r.shape[1]
    count = GROUPS // pieces

    def whole_piece(k):
        for g in range(k * count, (k + 1) * count):
            whole(g)

    def drained(buf, a_s, a_r, d_s, d_r):
        sent(buf.at[c, pl.ds(0, n - 1)], a_s, a_r)
        sent(buf.at[c], d_s, d_r)

    spread(
        gall, ga_s, ga_r, gd_s, gd_r, [(0.1 * k, functools.partial(whole_piece, k)) for k in range(pieces)],
        [(0.11, lambda: finish(7)), (0.12, lambda: weight_lines(2)), (4.0, lambda: weight_lines(3))],
    )
    sent(rs1.at[:, others], r1_s, r1_r.at[0])
    sent(rsb.at[:, others], rb_s, rb_r.at[0])
    for p in range(n):
        @pl.when(b == p)
        def _():
            sent(s1b.at[pl.ds(0, early - owned(p))], r2_s, r2_r.at[0])
            if owned(p):
                sent(gall.at[c, a, pl.ds(0, (n - 1) * owned(p))], gb_s, gb_r.at[0])

    arrived(gall.at[other], gd_s, gd_r)

    slots = ((0, 0), (0, 0), *(((1, nx - 1),) * 4), (2, 2), (2, 2))
    arrived(left.at[pl.ds(1, nx - 1)], lx_s, lx_r)
    rows = left.shape[2]
    left_done = jnp.zeros((n * rows, 2 * value_width), jnp.float32)
    for g in range(GROUPS):
        columns = [
            left[slots[g][i], :, :, CHUNK[g][i] * ch : (CHUNK[g][i] + 1) * ch].reshape(n * rows, ch) for i in range(2)
        ]
        grown = gall[:, :, g].reshape(2 * value_width, 2 * ch)
        left_done = left_done + dot(jnp.concatenate(columns, axis=1), grown, NT)

    high = left_done.astype(jnp.bfloat16)
    rest = left_done - high.astype(jnp.float32)
    middle = rest.astype(jnp.bfloat16)
    low = (rest - middle.astype(jnp.float32)).astype(jnp.bfloat16)
    done = []
    for h in range(2):
        columns = slice(h * value_width, (h + 1) * value_width)
        root = right[columns, :]
        done.append(dot(high[:, columns], root) + (dot(middle[:, columns], root) + dot(low[:, columns], root)))
    preconditioned = jnp.concatenate(done, axis=1)
    grown_line[...] = preconditioned.reshape(grown_line.shape)
    fresh = momentum_decay * momentum[...] + (1.0 - momentum_decay) * preconditioned.reshape(grown_line.shape)
    mall[c, a] = fresh.astype(jnp.bfloat16)

    def offered(value, slots, send, recv, where, at, size):
        slots[at] = value
        for d in range(1, size):
            start(slots.at[at], slots.at[at], send, recv, where(around(at + d, size)))

    stages = (
        (ssx, sx_s, sx_r, at_x, x, nx), (ssa, sa_s, sa_r, at_a, a, n), (ssd, sd_s, sd_r, lambda p: partner, c, 2),
    )
    squares = jnp.sum(jnp.sum(fresh * fresh, axis=0), keepdims=True)
    offered(jnp.broadcast_to(squares, ssx.shape[1:]), *stages[0])
    total = []

    def pass_on(index):
        slots, send, recv, _, _, size = stages[index]
        arrived(slots.at[pl.ds(0, size - 1)], send, recv)
        squares = jnp.sum(slots[...], axis=0)
        if index + 1 < len(stages):
            offered(squares, *stages[index + 1])
        else:
            total.append(squares)

    spread(
        mall, ma_s, ma_r, md_s, md_r, [(0.35 * k, lambda: None) for k in range(ma_r.shape[1])],
        [(4.7, lambda: weight_lines(4)), *((when, functools.partial(pass_on, index)) for index, when in enumerate((2.8, 6.6, 9.3)))],
    )
    factor = clip_level * lax.rsqrt(total[0] / entries + epsilon)
    factor_out[...] = jnp.broadcast_to(factor[0:1, 0:1], factor_out.shape)
    grown_out[...] = grown_line[b]
    arrived(wall.at[other], wd_s, wd_r)
    scale = factor[0:1, 0:1].reshape(1, 1, 1)

    def final(core, line):
        held = wall[core, line]
        step = scale * mall[core, line].astype(jnp.float32) + weight_decay * held
        return (held - step_rate * step).astype(jnp.bfloat16)

    arrived(mall.at[other], md_s, md_r)

    def laid(i, carry):
        copy_out[i, :, 0] = final(0, i)
        copy_out[:, i, 1] = final(1, i)
        return carry

    lax.fori_loop(0, n, laid, 0)
    drained(gall, ga_s, ga_r.at[0, 0], gd_s, gd_r)
    drained(mall, ma_s, ma_r.at[0, 0], md_s, md_r)
    sent(left.at[pl.ds(1, nx - 1)], lx_s, lx_r)
    drained(wall, wa_s, wa_r.at[0], wd_s, wd_r)
    for slots, send, recv, _, _, size in stages:
        sent(slots.at[pl.ds(0, size - 1)], send, recv)


def local(
    query_one, key_one, query_two, key_two, values, mix_ratio, head_gain,
    cotangent, left_roots, right_roots, weight, momentum,
):
    n = lax.axis_size("fs_0")
    nx = lax.axis_size("tp")
    tokens, own_cols = cotangent.shape
    rows = weight.shape[0]
    width = values.shape[1] // 2
    parts = width // n
    pair = own_cols // 2
    bf16, f32 = jnp.bfloat16, jnp.float32
    dma = pltpu.SemaphoreType.DMA
    vmem = pl.BlockSpec(memory_space=pltpu.VMEM)
    hbm = pl.BlockSpec(memory_space=pltpu.HBM)
    tile = (8, 128)
    shapes = pltpu.VMEM
    gain, mix = head_gain.reshape(1, -1), mix_ratio.reshape(1, -1)
    scratch = [
        shapes(array.shape, array.dtype)
        for array in (query_one, key_one, query_two, key_two, values, mix, gain, cotangent, right_roots)
    ]
    scratch += [
        dma((12,)),
        shapes((GROUPS - 2, tokens, pair), bf16),
        shapes((GROUPS, tokens, pair), bf16),
        shapes((width, tokens), bf16),
        shapes((width, tokens), bf16),
        shapes((width, tokens), bf16),
        shapes((GROUPS, n, parts, pair), bf16),
        shapes((GROUPS, n, parts, pair), bf16),
        shapes((GROUPS, parts, pair), bf16),
        shapes((n, GROUPS // n, parts, pair), bf16),
        shapes((LAST, n, parts, pair), bf16),
        shapes((2, n, GROUPS, parts, pair), bf16),
        shapes((2, n, n, rows, own_cols), f32),
        shapes((2, n, n, rows, own_cols), bf16),
        shapes((nx, *tile), f32),
        shapes((n, *tile), f32),
        shapes((2, *tile), f32),
        shapes((nx, n, rows, own_cols), bf16),
        shapes((n, rows, own_cols), f32),
        shapes((n, rows, own_cols), f32),
    ]
    pieces = min(4, n)
    for received in (
        (GROUPS - 2,), (GROUPS,), (), (GROUPS,), (GROUPS // n,), (LAST,), (GROUPS,), (n - 1, pieces), (), (n - 1, pieces), (),
        (), (n - 1,), (), (), (), (), (), (), (),
    ):
        scratch += [dma, dma(received) if received else dma]
    inputs = [
        pltpu.with_memory_space_constraint(array, pltpu.HBM)
        for array in (
            query_one, key_one, query_two, key_two, values, mix, gain,
            cotangent, left_roots, right_roots, weight, momentum,
        )
    ]
    grown, factor, copied = pl.pallas_call(
        functools.partial(kernel, float(weight.size * n * n * 2 * nx)),
        out_shape=(
            jax.ShapeDtypeStruct(weight.shape, f32),
            jax.ShapeDtypeStruct(weight.shape, f32),
            jax.ShapeDtypeStruct((n, n, 2, rows, own_cols), bf16),
        ),
        in_specs=[hbm] * 12,
        out_specs=[vmem] * 3,
        scratch_shapes=scratch,
        compiler_params=pltpu.CompilerParams(
            collective_id=0, has_side_effects=True, vmem_limit_bytes=40 * 1024 * 1024
        ),
    )(*inputs)
    momentum_new = momentum_decay * momentum + (1.0 - momentum_decay) * grown
    step = factor * momentum_new + weight_decay * weight
    weight_new = weight - step_rate * step
    return step, weight_new, momentum_new, copied.reshape(-1, own_cols)


def split_mesh(mesh):
    lines = int((mesh.shape["fs"] // 2) ** 0.5)
    return Mesh(mesh.devices.reshape(lines, lines, 2, mesh.shape["tp"]), (*FS, "tp"))


def solution(mesh):
    return jax.shard_map(
        local,
        mesh=split_mesh(mesh),
        in_specs=(
            P(FS, "tp"), P(FS, "tp"), P(FS, "tp"), P(FS, "tp"), P(FS, "tp"), P("tp"), P(),
            P(FS, "tp"), P(FS, None), P("tp", None), P(FS, "tp"), P(FS, "tp"),
        ),
        out_specs=(P(FS, "tp"), P(FS, "tp"), P(FS, "tp"), P(None, "tp")),
        check_vma=False,
    )
```
